32 devices in a mesh: grp: 2 (over y), fs: 4 (over z), tp: 4 (over x, core).
Axes of the slice: x: 2, y: 2, z: 4, core: 2. Of those that a mesh axis runs over, the one named last changes fastest.
Arguments:
- prompt: bfloat16 [8, 1024, 2048], P(('grp', 'tp')), parts along dimension 0, may hold values from -6 to 6
- gate_first: float32 [2048, 5632], P('fs', 'tp'), may hold values from -0.125 to 0.125
- up_first: float32 [2048, 5632], P('fs', 'tp'), may hold values from -0.125 to 0.125
- down_first: float32 [5632, 2048], P('fs', 'tp'), may hold values from -0.3125 to 0.3125
- norm_gain: float32 [2048], replicated, may hold values from 0.1 to 1.9
- gate_second: float32 [2048, 5632], P('fs', 'tp'), may hold values from -0.125 to 0.125
- up_second: float32 [2048, 5632], P('fs', 'tp'), may hold values from -0.125 to 0.125
- down_second: float32 [5632, 2048], P('fs', 'tp'), may hold values from -0.3125 to 0.3125
Outputs:
- result: bfloat16 [8, 1024, 2048], P(('grp', 'tp'), 'fs'), parts along dimension 0
- gate_one: bfloat16 [4096, 5632], P('grp', 'fs'), parts along dimension 0
- up_one: bfloat16 [4096, 5632], P('grp', 'fs'), parts along dimension 0
- down_one: bfloat16 [5632, 4096], P('fs', 'grp'), parts along dimension 1
- gate_two: bfloat16 [4096, 5632], P('grp', 'fs'), parts along dimension 0
- up_two: bfloat16 [4096, 5632], P('grp', 'fs'), parts along dimension 0
- down_two: bfloat16 [5632, 4096], P('fs', 'grp'), parts along dimension 1
The draws below stay inside these ranges and needn't reach their ends.
There are 2 independent parts, one for each index of `grp`. The reference program is written for one: setup_inputs(seed, part) draws one part's arguments, and reference() takes and returns one part's arrays. A program takes and returns all parts, laid end to end along the dimension named above; an argument that names none is the same for every part. Nothing has to cross between parts.
All inputs are finite; a program needn't handle non-finite values.
Results may differ from the reference program's by a relative error of at most 0.029.
Values may be sent and summed in bfloat16 or wider, within the bound.
A program may use at most 192 MiB of HBM per device.

```python
import jax
import jax.numpy as jnp
from jax import lax

D = 2048
FF = 5632
LENGTH = 1024
PROMPTS = 4
N_FS = 4


def block_levels(rng, shape, pieces, least, largest):
    factor_of = 1.0
    for axis_at, blocks in pieces:
        heights = jax.random.uniform(jax.random.fold_in(jax.random.fold_in(rng, 6), axis_at), (blocks,), jnp.float32, least / len(pieces), largest / len(pieces))
        factor_of = factor_of * jnp.repeat(jnp.exp(heights), shape[axis_at] // blocks).reshape((-1,) + (1,) * (len(shape) - 1 - axis_at))
    return factor_of


def bell_draw(key, extent, scale, bound, shards=(), kind=jnp.bfloat16):
    loudness = block_levels(key, extent, shards, -0.22, 0.18) if shards else 1.0
    entries = jax.random.normal(key, extent, jnp.float32) * scale * loudness
    return jnp.minimum(jnp.maximum(entries, -bound), bound).astype(kind)


def setup_inputs(seed: int = 0, part: int = 0) -> dict:
    seeds = jax.random.split(jax.random.key(seed), 9)
    part_keys = jax.random.split(jax.random.fold_in(seeds[8], part), 9)
    prompt = bell_draw(part_keys[0], (PROMPTS, LENGTH, D), 1.0, 6.0, ((0, 4),))
    gate_first = bell_draw(seeds[1], (D, FF), D ** -0.5, 0.125, ((0, 4), (1, 4)), jnp.float32)
    up_first = bell_draw(seeds[2], (D, FF), D ** -0.5, 0.125, ((0, 4), (1, 4)), jnp.float32)
    down_first = bell_draw(seeds[3], (FF, D), (4.0 * FF ** -0.5), 0.3125, ((0, 4), (1, 4)), jnp.float32)
    norm_gain = jnp.clip(1.0 + 0.18 * jax.random.normal(seeds[4], (D,), jnp.float32), 0.1, 1.9)
    gate_second = bell_draw(seeds[5], (D, FF), D ** -0.5, 0.125, ((0, 4), (1, 4)), jnp.float32)
    up_second = bell_draw(seeds[6], (D, FF), D ** -0.5, 0.125, ((0, 4), (1, 4)), jnp.float32)
    down_second = bell_draw(seeds[7], (FF, D), (4.0 * FF ** -0.5), 0.3125, ((0, 4), (1, 4)), jnp.float32)
    return dict(prompt=prompt, gate_first=gate_first, up_first=up_first, down_first=down_first, norm_gain=norm_gain, gate_second=gate_second, up_second=up_second, down_second=down_second)


norm_eps = 1e-05
deep_alpha = 2.0 ** 0.25
half_step = 0.5

def plain_norm(values):
    row_mean = lax.optimization_barrier(jnp.mean(values, axis=-1, keepdims=True))
    centred = values - row_mean
    variance = lax.optimization_barrier(jnp.mean(centred * centred, axis=-1, keepdims=True))
    return centred * lax.rsqrt(variance + norm_eps)

def gated_hidden(inputs, gate_proj, up_proj):
    gate_act = jnp.dot(inputs, gate_proj, preferred_element_type=jnp.float32)
    up_act = jnp.dot(inputs, up_proj, preferred_element_type=jnp.float32)
    return (jax.nn.silu(gate_act) * up_act).astype(jnp.bfloat16)

def block_sums(hidden, down_proj):
    block_width = hidden.shape[1] // N_FS

    def one_block(carried, block_index):
        hidden_block = lax.dynamic_slice_in_dim(hidden, block_index * block_width, block_width, 1)
        down_block = lax.dynamic_slice_in_dim(down_proj, block_index * block_width, block_width, 0)
        partial_term = jnp.dot(hidden_block, down_block, preferred_element_type=jnp.float32).astype(jnp.bfloat16)
        partial_term = lax.optimization_barrier(partial_term)
        return (carried + partial_term.astype(jnp.float32), None)
    start_sum = jnp.zeros((hidden.shape[0], down_proj.shape[1]), jnp.float32)
    summed, unused = lax.scan(one_block, start_sum, jnp.arange(N_FS, dtype=jnp.int32))
    return summed

def reference(prompt, gate_first, up_first, down_first, norm_gain, gate_second, up_second, down_second):
    gate_one = gate_first.astype(jnp.bfloat16)
    up_one = up_first.astype(jnp.bfloat16)
    down_one = down_first.astype(jnp.bfloat16)
    gate_two = (norm_gain[:, None] * gate_second).astype(jnp.bfloat16)
    up_two = (norm_gain[:, None] * up_second).astype(jnp.bfloat16)
    down_two = down_second.astype(jnp.bfloat16)
    tokens = prompt.reshape(-1, prompt.shape[-1])
    hidden_one = gated_hidden(tokens, gate_one, up_one)
    ffn_one = block_sums(hidden_one, down_one)
    normed_one = plain_norm(deep_alpha * tokens.astype(jnp.float32) + half_step * ffn_one).astype(jnp.bfloat16)
    hidden_two = gated_hidden(normed_one, gate_two, up_two)
    ffn_two = block_sums(hidden_two, down_two)
    residual_two = deep_alpha * norm_gain * normed_one.astype(jnp.float32)
    result = plain_norm(residual_two + half_step * ffn_two).astype(jnp.bfloat16).reshape(prompt.shape)
    return (result, gate_one, up_one, down_one, gate_two, up_two, down_two)
```

```python
import jax
import jax.numpy as jnp
from jax import lax
from jax.experimental import pallas as pl
from jax.experimental.pallas import tpu as pltpu
from jax.sharding import PartitionSpec as P

norm_eps = 1e-05
deep_alpha = 2.0**0.25
half_step = 0.5
lane = 128
steps = 8
MESH = pl.DeviceIdType.MESH
ANY = pl.BlockSpec(memory_space=pl.ANY)
VMEM = pl.BlockSpec(memory_space=pltpu.VMEM)


def plain_norm(values):
    row_mean = jnp.mean(values, axis=-1, keepdims=True)
    centred = values - row_mean
    variance = jnp.mean(centred * centred, axis=-1, keepdims=True)
    return centred * lax.rsqrt(variance + norm_eps)


def gated_hidden(inputs, gate_proj, up_proj):
    gate_act = jnp.dot(inputs, gate_proj, preferred_element_type=jnp.float32)
    up_act = jnp.dot(inputs, up_proj, preferred_element_type=jnp.float32)
    return (jax.nn.silu(gate_act) * up_act).astype(jnp.bfloat16)


def relay_weights(gate_proj, up_proj, down_proj):
    gate_rows, up_rows, down_mine = (
        lax.all_gather(gate_proj, "tp", axis=1, tiled=True),
        lax.all_gather(up_proj, "tp", axis=1, tiled=True),
        lax.all_gather(down_proj, "tp", axis=1, tiled=True),
    )
    gate_mine, up_mine = (
        lax.all_to_all(gate_rows, "fs", split_axis=1, concat_axis=0, tiled=True),
        lax.all_to_all(up_rows, "fs", split_axis=1, concat_axis=0, tiled=True),
    )
    return (gate_mine, up_mine, down_mine)


def general_blocks(tokens, norm_gain, first, second):
    fs_index, fs_count = lax.axis_index("fs"), lax.axis_size("fs")
    own_count = tokens.shape[0] // fs_count

    def summed(rows, projs):
        terms = jnp.dot(
            gated_hidden(rows, projs[0], projs[1]), projs[2], preferred_element_type=jnp.float32
        ).astype(jnp.bfloat16)
        parts = lax.all_to_all(
            terms.reshape(fs_count, own_count, -1), "fs", split_axis=0, concat_axis=0
        )
        return jnp.sum(parts.astype(jnp.float32), axis=0)

    own_tokens = lax.dynamic_slice_in_dim(tokens, fs_index * own_count, own_count, 0)
    first = relay_weights(*first)
    second = relay_weights(*second)
    normed_own = plain_norm(
        deep_alpha * own_tokens.astype(jnp.float32) + half_step * summed(tokens, first)
    ).astype(jnp.bfloat16)
    normed = lax.all_gather(normed_own, "fs", axis=0, tiled=True)
    ffn_two = summed(normed, second)
    residual_two = deep_alpha * norm_gain * normed_own.astype(jnp.float32)
    return (plain_norm(residual_two + half_step * ffn_two).astype(jnp.bfloat16), *first, *second)


class Here:
    def __init__(self):
        self.g, self.f, self.t = (lax.axis_index(name) for name in ("grp", "fs", "tp"))
        side = lax.axis_size("tp")
        self.side = side
        self.x, self.c = self.t // 2, self.t % 2
        self.q = self.g * 2 + self.x
        self.xt = (self.t + 2) % side
        self.ct = self.t + 1 - 2 * self.c
        self.xn = (self.g, self.f, self.xt)
        self.yn = (1 - self.g, self.f, self.t)
        self.cn = (self.g, self.f, self.ct)
        last = lax.axis_size("fs") - 1
        self.m = self.f // 2
        self.end = self.f + self.m * (last - 2 * self.f)
        self.inner = (self.g, self.f + 1 - 2 * self.m, self.t)
        self.outer = (self.g, self.f - 1 + 2 * self.m, self.t)
        self.last = last

    def owner(self, mirrored):
        return mirrored + self.m * (self.last - 2 * mirrored)

    def order(self, k):
        f = self.f
        return (f, f + 1 - 2 * (f % 2), (f + 2) % self.side, self.last - f)[k]


def remote(src, dst, send_sem, recv_sem, device):
    return pltpu.make_async_remote_copy(
        src_ref=src,
        dst_ref=dst,
        send_sem=send_sem,
        recv_sem=recv_sem,
        device_id=device,
        device_id_type=MESH,
    )


class PlaneGather:
    kinds = 9

    def __init__(self, here, w, sems):
        self.h, self.w, self.sems = here, w, sems
        self.rows = w.shape[1] // here.side
        self.piece = self.rows // 4
        self.cut = self.piece * 3 // 4
        self.started = []

    def region(self, which, z, q, first, count):
        return self.w.at[which, pl.ds(z * self.rows + q * self.piece + first, count)]

    def send(self, z, kind, region, device):
        copy = remote(region, region, self.sems.at[0, z, kind], self.sems.at[1, z, kind], device)
        copy.start()
        self.started.append(copy)

    def arrive(self, z, kind, region):
        remote(
            region, region, self.sems.at[0, z, kind], self.sems.at[1, z, kind], self.h.cn
        ).wait_recv()

    def own(self, k):
        h, z = self.h, self.h.order(k)
        region = self.region(h.c, z, h.q, 0, self.piece)
        self.send(z, 0, region, h.xn)
        self.send(z, 1, region, h.yn)
        self.send(z, 4, region, h.cn)

    def quarters(self):
        h = self.h
        return (h.g * 2 + 1 - h.x, (1 - h.g) * 2 + h.x, (1 - h.g) * 2 + 1 - h.x)

    def forward(self, k):
        h, z = self.h, self.h.order(k)
        from_x, from_y, unused = self.quarters()
        region = self.region(h.c, z, from_x, 0, self.piece)
        self.arrive(z, 0, region)
        self.send(z, 2, self.region(h.c, z, from_x, 0, self.cut), h.yn)
        self.send(z, 5, region, h.cn)
        region = self.region(h.c, z, from_y, 0, self.piece)
        self.arrive(z, 1, region)
        self.send(z, 3, self.region(h.c, z, from_y, self.cut, self.piece - self.cut), h.xn)
        self.send(z, 6, region, h.cn)

    def corner(self, k):
        h, z = self.h, self.h.order(k)
        across = self.quarters()[2]
        region = self.region(h.c, z, across, 0, self.cut)
        self.arrive(z, 2, region)
        self.send(z, 7, region, h.cn)
        region = self.region(h.c, z, across, self.cut, self.piece - self.cut)
        self.arrive(z, 3, region)
        self.send(z, 8, region, h.cn)

    def finish(self):
        h, other = self.h, 1 - self.h.c
        from_x, from_y, across = self.quarters()
        for k in range(h.side):
            z = h.order(k)
            self.arrive(z, 4, self.region(other, z, h.q, 0, self.piece))
            self.arrive(z, 5, self.region(other, z, from_x, 0, self.piece))
            self.arrive(z, 6, self.region(other, z, from_y, 0, self.piece))
            self.arrive(z, 7, self.region(other, z, across, 0, self.cut))
            self.arrive(z, 8, self.region(other, z, across, self.cut, self.piece - self.cut))
        for copy in self.started:
            copy.wait_send()


class DownGather:
    kinds = 5

    def __init__(self, here, src, dst, sems, bounce, local):
        self.h, self.src, self.dst, self.sems = here, src, dst, sems
        self.bounce, self.local = bounce, local
        self.rows, self.cols = src.shape
        self.half = self.rows // 2
        self.started = []

    def columns(self, t):
        return pl.ds(pl.multiple_of(t * self.cols, self.cols), self.cols)

    def part(self, g, t):
        return self.dst.at[pl.ds(g * self.half, self.half), self.columns(t)]

    def send(self, kind, src, dst, device):
        copy = remote(src, dst, self.sems.at[0, kind], self.sems.at[1, kind], device)
        copy.start()
        self.started.append(copy)

    def arrive(self, kind, region):
        remote(
            region, region, self.sems.at[0, kind], self.sems.at[1, kind], self.h.cn
        ).wait_recv()

    def begin(self):
        h = self.h
        self.take = pltpu.make_async_copy(self.src, self.bounce, self.local.at[0])
        self.take.start()
        self.send(
            0, self.src.at[pl.ds(h.g * self.half, self.half)], self.part(h.g, h.t), h.xn
        )
        self.send(2, self.src, self.dst.at[:, self.columns(h.t)], h.cn)

    def place(self):
        self.take.wait()
        self.put = pltpu.make_async_copy(
            self.bounce, self.dst.at[:, self.columns(self.h.t)], self.local.at[1]
        )
        self.put.start()

    def forward(self):
        h = self.h
        region = self.part(h.g, h.xt)
        self.arrive(0, region)
        self.send(1, region, region, h.yn)
        self.send(3, region, region, h.cn)

    def corner(self):
        h = self.h
        region = self.part(1 - h.g, h.xt)
        self.arrive(1, region)
        self.send(4, region, region, h.cn)

    def finish(self):
        h = self.h
        across = (h.ct + 2) % h.side
        self.arrive(2, self.dst.at[:, self.columns(h.ct)])
        self.arrive(3, self.part(h.g, across))
        self.arrive(4, self.part(1 - h.g, across))
        self.put.wait()
        for copy in self.started:
            copy.wait_send()


class Placement:
    def __init__(self, here, src, dst, send_sem, recv_sem, bounce, local):
        self.h, self.src, self.dst = here, src, dst
        self.send_sem, self.recv_sem, self.bounce, self.local = send_sem, recv_sem, bounce, local
        self.rows = src.shape[1]
        self.piece = self.rows // 4

    def copies(self):
        h = self.h
        for x in range(2):
            for c in range(2):
                target, q = 2 * x + c, h.g * 2 + x
                mine = jnp.logical_and(h.f == h.t, h.t == target)
                src = self.src.at[c, pl.ds(q * self.piece, self.piece)]
                dst = self.dst.at[c, pl.ds(h.f * self.rows + q * self.piece, self.piece)]
                copy = remote(
                    src, dst, self.send_sem.at[target], self.recv_sem.at[h.f], (h.g, h.t, target)
                )
                yield mine, src, dst, copy

    def begin(self):
        for mine, src, dst, copy in self.copies():

            @pl.when(jnp.logical_not(mine))
            def _():
                copy.start()

            @pl.when(mine)
            def _():
                take = pltpu.make_async_copy(src, self.bounce, self.local)
                take.start()
                take.wait()
                put = pltpu.make_async_copy(self.bounce, dst, self.local)
                put.start()
                put.wait()

    def arrived(self, k):
        h = self.h
        z = h.order(k)
        region = self.dst.at[h.c, pl.ds(z * self.rows + h.q * self.piece, self.piece)]
        copy = remote(region, region, self.send_sem.at[0], self.recv_sem.at[z], h.cn)
        if k == 0:

            @pl.when(h.f != h.t)
            def _():
                copy.wait_recv()

        else:
            copy.wait_recv()

    def finish(self):
        for mine, src, dst, copy in self.copies():

            @pl.when(jnp.logical_not(mine))
            def _():
                copy.wait_send()


def weights_kernel(
    src_one, down_src, src_two, w_one, down_one, w_two,
    bounce, down_bounce, place_sems, plane_sems, down_sems, local,
):
    h = Here()
    first = Placement(
        h, src_one, w_one, place_sems.at[0, 0], place_sems.at[0, 1], bounce, local.at[2]
    )
    second = Placement(
        h, src_two, w_two, place_sems.at[1, 0], place_sems.at[1, 1], bounce, local.at[2]
    )
    gather = PlaneGather(h, w_one, plane_sems)
    down = DownGather(h, down_src, down_one, down_sems, down_bounce, local)
    first.begin()
    down.begin()
    down.place()
    for k in range(h.side):
        first.arrived(k)
        gather.own(k)
        if k == 1:
            down.forward()
        if k >= 1:
            gather.forward(k - 1)
        if k >= 2:
            gather.corner(k - 2)
        if k == 2:
            second.begin()
            down.corner()
    gather.forward(h.side - 1)
    gather.corner(h.side - 2)
    gather.corner(h.side - 1)
    gather.finish()
    down.finish()
    for k in range(h.side):
        second.arrived(k)
    first.finish()
    second.finish()


def gather_weights(src_one, down_src, src_two):
    side = lax.axis_size("tp")
    two, rows, width = src_one.shape
    full = jax.ShapeDtypeStruct((two, rows * side, width), src_one.dtype)
    down = jax.ShapeDtypeStruct((down_src.shape[0], down_src.shape[1] * side), down_src.dtype)
    return pl.pallas_call(
        weights_kernel,
        out_shape=(full, down, full),
        in_specs=[ANY] * 3,
        out_specs=(ANY,) * 3,
        scratch_shapes=[
            pltpu.VMEM((rows // 4, width), src_one.dtype),
            pltpu.VMEM(down_src.shape, down_src.dtype),
            pltpu.SemaphoreType.DMA((2, 2, side)),
            pltpu.SemaphoreType.DMA((2, side, PlaneGather.kinds)),
            pltpu.SemaphoreType.DMA((2, DownGather.kinds)),
            pltpu.SemaphoreType.DMA((3,)),
        ],
        compiler_params=pltpu.CompilerParams(has_side_effects=True),
        name="gather_weights",
    )(src_one, down_src, src_two)


def compute_kernel(
    tokens, w, down, terms, gate_out, up_out, down_out,
    rows_in, w_in, down_in, hidden, terms_in, sems,
):
    groups = w.shape[2] // lane
    wide = 2 * lane
    spans = down.shape[1] // wide
    count = tokens.shape[0]
    block = count // 4

    def w_load(which, j):
        return pltpu.make_async_copy(
            w.at[which, :, pl.ds(pl.multiple_of(j * lane, lane), lane)],
            w_in.at[j, :, pl.ds(which * lane, lane)],
            sems.at[which, j],
        )

    def w_store(which, j):
        return pltpu.make_async_copy(
            w_in.at[j, :, pl.ds(which * lane, lane)],
            (gate_out, up_out)[which].at[:, pl.ds(pl.multiple_of(j * lane, lane), lane)],
            sems.at[2 + which, j],
        )

    take_rows = pltpu.make_async_copy(tokens, rows_in, sems.at[4, 0])
    take_down = pltpu.make_async_copy(down, down_in, sems.at[4, 1])
    give_down = pltpu.make_async_copy(down_in, down_out, sems.at[4, 2])
    take_rows.start()

    @pl.loop(0, groups)
    def _(j):
        w_load(0, j).start()
        w_load(1, j).start()

    take_down.start()
    take_rows.wait()

    @pl.loop(0, groups)
    def _(j):
        w_load(0, j).wait()
        w_load(1, j).wait()
        w_store(0, j).start()
        w_store(1, j).start()

        @pl.loop(0, 4)
        def _(r):
            at = pl.ds(pl.multiple_of(r * block, block), block)
            act = jnp.dot(rows_in[at, :], w_in[j], preferred_element_type=jnp.float32)
            gate_act, up_act = act[:, :lane], act[:, lane:]
            value = gate_act / (1.0 + jnp.exp(-gate_act)) * up_act
            hidden[at, pl.ds(pl.multiple_of(j * lane, lane), lane)] = value.astype(jnp.bfloat16)

    take_down.wait()
    give_down.start()

    @pl.loop(0, spans)
    def _(n):
        cols = pl.ds(pl.multiple_of(n * wide, wide), wide)

        @pl.loop(0, 4)
        def _(r):
            at = pl.ds(pl.multiple_of(r * block, block), block)
            terms_in[at, cols] = jnp.dot(
                hidden[at, :], down_in[:, cols], preferred_element_type=jnp.float32
            ).astype(jnp.bfloat16)

    give_terms = pltpu.make_async_copy(terms_in, terms, sems.at[4, 3])
    give_terms.start()

    @pl.loop(0, groups)
    def _(j):
        w_store(0, j).wait()
        w_store(1, j).wait()

    give_down.wait()
    give_terms.wait()


def compute_terms(tokens, w, down):
    two, depth, width = w.shape
    count = tokens.shape[0]
    groups = width // lane
    proj = jax.ShapeDtypeStruct((depth, width), w.dtype)
    flops = 2 * count * depth * width * 3
    return pl.pallas_call(
        compute_kernel,
        out_shape=(
            jax.ShapeDtypeStruct((count, down.shape[1]), jnp.bfloat16),
            proj,
            proj,
            jax.ShapeDtypeStruct(down.shape, down.dtype),
        ),
        in_specs=[ANY] * 3,
        out_specs=(ANY,) * 4,
        scratch_shapes=[
            pltpu.VMEM(tokens.shape, tokens.dtype),
            pltpu.VMEM((groups, depth, 2 * lane), w.dtype),
            pltpu.VMEM(down.shape, down.dtype),
            pltpu.VMEM((count, width), jnp.bfloat16),
            pltpu.VMEM((count, down.shape[1]), jnp.bfloat16),
            pltpu.SemaphoreType.DMA((5, max(groups, 4))),
        ],
        compiler_params=pltpu.CompilerParams(vmem_limit_bytes=56 * 1024 * 1024),
        cost_estimate=pl.CostEstimate(flops=flops, bytes_accessed=6 * w.size, transcendentals=0),
        name="compute_terms",
    )(tokens, w, down)


class LineSum:
    kinds = 6

    def __init__(self, here, terms, from_outer, from_inner, from_middle, to_inner, to_outer, sems):
        self.h, self.terms = here, terms
        self.from_outer, self.from_inner, self.from_middle = from_outer, from_inner, from_middle
        self.to_inner, self.to_outer, self.sems = to_inner, to_outer, sems
        self.own = terms.shape[0] // (here.last + 1)
        self.size = self.own // steps

    def term(self, mirrored, s):
        first = self.h.owner(mirrored) * self.own + s * self.size
        return pl.ds(pl.multiple_of(first, self.size), self.size)

    def at(self, s):
        return pl.ds(pl.multiple_of(s * self.size, self.size), self.size)

    def copy(self, src, dst, kind, s, device):
        return remote(src, dst, self.sems.at[0, kind, s], self.sems.at[1, kind, s], device)

    def start_copy(self, o, s):
        slot = 3 - o
        return self.copy(
            self.terms.at[self.term(o, s)], self.from_outer.at[slot, self.at(s)], slot, s,
            self.h.inner,
        )

    def middle_copy(self, o, s):
        slot = 3 - o
        return self.copy(
            self.to_inner.at[slot, self.at(s)], self.from_middle.at[slot, self.at(s)], 3 + slot,
            s, self.h.inner,
        )

    def back_copy(self, s):
        return self.copy(
            self.to_outer.at[self.at(s)], self.from_inner.at[self.at(s)], 5, s, self.h.outer
        )

    def send_start(self, s):
        for o in (3, 2, 1):
            self.start_copy(o, s).start()

    def relay(self, s):
        at = self.at(s)
        for o in (3, 2):
            slot = 3 - o
            self.start_copy(o, s).wait_recv()
            self.to_inner[slot, at, :] = (
                self.from_outer[slot, at, :].astype(jnp.float32)
                + self.terms[self.term(o, s), :].astype(jnp.float32)
            ).astype(jnp.bfloat16)
            self.middle_copy(o, s).start()

    def relay_back(self, s):
        at = self.at(s)
        self.middle_copy(3, s).wait_recv()
        self.to_outer[at, :] = (
            self.from_middle[0, at, :].astype(jnp.float32)
            + self.terms[self.term(0, s), :].astype(jnp.float32)
        ).astype(jnp.bfloat16)
        self.back_copy(s).start()

    def inner_total(self, s):
        at = self.at(s)
        self.start_copy(1, s).wait_recv()
        self.middle_copy(2, s).wait_recv()
        return (
            self.from_outer[2, at, :].astype(jnp.float32)
            + self.terms[self.term(1, s), :].astype(jnp.float32)
        ) + self.from_middle[1, at, :].astype(jnp.float32)

    def end_total(self, s):
        at = self.at(s)
        self.back_copy(s).wait_recv()
        return self.terms[self.term(0, s), :].astype(jnp.float32) + self.from_inner[
            at, :
        ].astype(jnp.float32)

    def finish_end(self, s):
        for o in (3, 2, 1):
            self.start_copy(o, s).wait_send()

    def finish_inner(self, s):
        self.middle_copy(3, s).wait_send()
        self.middle_copy(2, s).wait_send()
        self.back_copy(s).wait_send()


def line_scratch(own, width):
    def rows(*lead):
        return pltpu.VMEM((*lead, own, width), jnp.bfloat16)

    return [
        rows(3), rows(), rows(2), rows(2), rows(),
        pltpu.SemaphoreType.DMA((2, LineSum.kinds, steps)),
    ]


class LineSpread:
    kinds = 6

    def __init__(self, here, out, sems, own):
        self.h, self.out, self.sems, self.own = here, out, sems, own
        self.size = own // steps

    def rows(self, mirrored, s):
        first = self.h.owner(mirrored) * self.own + s * self.size
        return self.out.at[pl.ds(pl.multiple_of(first, self.size), self.size)]

    def copy(self, mirrored, kind, s, device, src=None):
        rows = self.rows(mirrored, s)
        return remote(
            rows if src is None else src, rows, self.sems.at[0, kind, s], self.sems.at[1, kind, s],
            device,
        )

    def in_zero(self, s, src=None):
        return self.copy(0, 0, s, self.h.inner, src)

    def cross_one(self, s, src=None):
        return self.copy(1, 1, s, self.h.inner, src)

    def cross_zero(self, s):
        return self.copy(0, 2, s, self.h.inner)

    def out_any(self, o, s, src=None):
        return self.copy(o, 2 + o, s, self.h.outer, src)


def middle_kernel(
    terms, tokens, w_in, down_src, gathered, w, down,
    own_rows, normed, down_bounce,
    from_outer, from_inner, from_middle, to_inner, to_outer, line_sems,
    spread_sems, plane_sems, down_sems, local,
):
    h = Here()
    own = normed.shape[0]
    size = own // steps
    is_end = h.end == 0
    is_inner = h.end == 1
    line = LineSum(h, terms, from_outer, from_inner, from_middle, to_inner, to_outer, line_sems)
    spread = LineSpread(h, gathered, spread_sems, own)
    gather = PlaneGather(h, w, plane_sems)
    down_part = DownGather(h, down_src, down, down_sems, down_bounce, local)
    take = pltpu.make_async_copy(
        tokens.at[pl.ds(pl.multiple_of(h.f * own, own), own)], own_rows, local.at[2]
    )
    take.start()

    @pl.when(is_end)
    def _():
        line.send_start(0)
        line.send_start(1)

    down_part.begin()
    for k in range(h.side):
        gather.own(k)
    down_part.place()
    take.wait()

    def keep(s, total):
        at = pl.ds(s * size, size)
        normed[at, :] = plain_norm(
            deep_alpha * own_rows[at, :].astype(jnp.float32) + half_step * total
        ).astype(jnp.bfloat16)
        return normed.at[at]

    def put_own(s):
        first = h.f * own + s * size
        return pltpu.make_async_copy(
            normed.at[pl.ds(s * size, size)],
            gathered.at[pl.ds(pl.multiple_of(first, size), size)],
            local.at[3 + s],
        )

    def hand_on(s):
        @pl.when(is_inner)
        def _():
            spread.in_zero(s).wait_recv()
            spread.cross_zero(s).start()
            spread.cross_one_in(s).wait_recv()
            spread.out_any(2, s).start()
            spread.cross_zero_in(s).wait_recv()
            spread.out_any(3, s).start()

    spread.cross_one_in = lambda s: spread.copy(2, 1, s, h.inner)
    spread.cross_zero_in = lambda s: spread.copy(3, 2, s, h.inner)

    jobs = {
        1: [lambda: gather.forward(0), down_part.forward],
        2: [lambda: gather.forward(1)],
        3: [lambda: gather.forward(2), down_part.corner],
        4: [lambda: gather.forward(3)],
        5: [lambda: gather.corner(0), lambda: gather.corner(1)],
        6: [lambda: gather.corner(2)],
        7: [lambda: gather.corner(3)],
    }
    for s in range(steps):

        @pl.when(is_inner)
        def _():
            line.relay(s)
            line.relay_back(s)
            src = keep(s, line.inner_total(s))
            spread.cross_one(s, src).start()
            spread.out_any(1, s, src).start()

        @pl.when(is_end)
        def _():
            if s + 2 < steps:
                line.send_start(s + 2)
            src = keep(s, line.end_total(s))
            spread.in_zero(s, src).start()

        put_own(s).start()
        if s >= 1:
            hand_on(s - 1)
        for job in jobs.get(s, ()):
            job()
    hand_on(steps - 1)
    gather.finish()
    down_part.finish()
    for s in range(steps):
        put_own(s).wait()

        @pl.when(is_end)
        def _():
            for o in (1, 2, 3):
                spread.out_any(o, s).wait_recv()
            line.finish_end(s)
            spread.in_zero(s).wait_send()

        @pl.when(is_inner)
        def _():
            line.finish_inner(s)
            spread.cross_one(s).wait_send()
            spread.cross_zero(s).wait_send()
            for o in (1, 2, 3):
                spread.out_any(o, s).wait_send()


def middle(terms, tokens, w, down_src):
    side = lax.axis_size("tp")
    count, width = terms.shape
    own = count // lax.axis_size("fs")
    down = jax.ShapeDtypeStruct((down_src.shape[0], down_src.shape[1] * side), down_src.dtype)
    return pl.pallas_call(
        middle_kernel,
        out_shape=(
            jax.ShapeDtypeStruct(terms.shape, terms.dtype),
            jax.ShapeDtypeStruct(w.shape, w.dtype),
            down,
        ),
        in_specs=[VMEM, ANY, ANY, ANY],
        out_specs=(ANY,) * 3,
        input_output_aliases={2: 1},
        scratch_shapes=[
            pltpu.VMEM((own, width), jnp.bfloat16),
            pltpu.VMEM((own, width), jnp.bfloat16),
            pltpu.VMEM(down_src.shape, down_src.dtype),
            *line_scratch(own, width),
            pltpu.SemaphoreType.DMA((2, LineSpread.kinds, steps)),
            pltpu.SemaphoreType.DMA((2, side, PlaneGather.kinds)),
            pltpu.SemaphoreType.DMA((2, DownGather.kinds)),
            pltpu.SemaphoreType.DMA((3 + steps,)),
        ],
        compiler_params=pltpu.CompilerParams(
            has_side_effects=True, vmem_limit_bytes=48 * 1024 * 1024
        ),
        name="sum_norm_spread",
    )(terms, tokens, w, down_src)


def last_kernel(
    terms, normed, gain, result,
    own_rows, from_outer, from_inner, from_middle, to_inner, to_outer, line_sems, local,
):
    h = Here()
    own = result.shape[0]
    size = own // steps
    is_end = h.end == 0
    is_inner = h.end == 1
    line = LineSum(h, terms, from_outer, from_inner, from_middle, to_inner, to_outer, line_sems)

    @pl.when(is_end)
    def _():
        for s in range(steps):
            line.send_start(s)

    take = pltpu.make_async_copy(
        normed.at[pl.ds(pl.multiple_of(h.f * own, own), own)], own_rows, local.at[0]
    )
    take.start()
    take.wait()

    def keep(s, total):
        at = pl.ds(s * size, size)
        residual = deep_alpha * gain[...] * own_rows[at, :].astype(jnp.float32)
        result[at, :] = plain_norm(residual + half_step * total).astype(jnp.bfloat16)

    for s in range(steps):

        @pl.when(is_inner)
        def _():
            line.relay(s)
            line.relay_back(s)
            keep(s, line.inner_total(s))

        @pl.when(is_end)
        def _():
            keep(s, line.end_total(s))

    for s in range(steps):

        @pl.when(is_end)
        def _():
            line.finish_end(s)

        @pl.when(is_inner)
        def _():
            line.finish_inner(s)


def last(terms, normed, gain):
    count, width = terms.shape
    own = count // lax.axis_size("fs")
    return pl.pallas_call(
        last_kernel,
        out_shape=jax.ShapeDtypeStruct((own, width), jnp.bfloat16),
        in_specs=[VMEM, ANY, VMEM],
        out_specs=VMEM,
        scratch_shapes=[
            pltpu.VMEM((own, width), jnp.bfloat16),
            *line_scratch(own, width),
            pltpu.SemaphoreType.DMA((1,)),
        ],
        compiler_params=pltpu.CompilerParams(
            has_side_effects=True, vmem_limit_bytes=48 * 1024 * 1024
        ),
        name="sum_norm_last",
    )(terms, normed, gain)


def body(prompt, gate_first, up_first, down_first, norm_gain, gate_second, up_second, down_second):
    side, groups, planes = lax.axis_size("tp"), lax.axis_size("grp"), lax.axis_size("fs")
    fs_index = lax.axis_index("fs")
    tokens = prompt.reshape(-1, prompt.shape[-1])
    row_block, width = gate_first.shape
    gain_rows = lax.dynamic_slice_in_dim(norm_gain, fs_index * row_block, row_block, 0)[:, None]
    down_a, down_b = down_first.astype(jnp.bfloat16), down_second.astype(jnp.bfloat16)
    planar = (
        groups == 2
        and side == 2 * groups
        and planes == side
        and row_block % (4 * 64) == 0
        and width % lane == 0
        and down_first.shape[0] % 32 == 0
        and down_first.shape[1] % lane == 0
        and tokens.shape[0] % (planes * steps * 16) == 0
        and tokens.shape[1] % (2 * lane) == 0
    )
    if planar:
        src_one = jnp.stack([gate_first.astype(jnp.bfloat16), up_first.astype(jnp.bfloat16)])
        src_two = jnp.stack(
            [
                (gain_rows * gate_second).astype(jnp.bfloat16),
                (gain_rows * up_second).astype(jnp.bfloat16),
            ]
        )
        w_one, down_one, w_two = gather_weights(src_one, down_a, src_two)
        terms_one, gate_one, up_one, down_one = compute_terms(tokens, w_one, down_one)
        normed, w_two, down_two = middle(terms_one, tokens, w_two, down_b)
        terms_two, gate_two, up_two, down_two = compute_terms(normed, w_two, down_two)
        result = last(terms_two, normed, norm_gain[None, :])
    else:
        result, gate_one, up_one, down_one, gate_two, up_two, down_two = general_blocks(
            tokens,
            norm_gain,
            (gate_first.astype(jnp.bfloat16), up_first.astype(jnp.bfloat16), down_a),
            (
                (gain_rows * gate_second).astype(jnp.bfloat16),
                (gain_rows * up_second).astype(jnp.bfloat16),
                down_b,
            ),
        )
    return (
        result.reshape(1, result.shape[0], result.shape[-1]),
        gate_one,
        up_one,
        down_one,
        gate_two,
        up_two,
        down_two,
    )


def solution(mesh):
    placed = (
        P(("grp", "tp"), None, None),
        P("fs", "tp"),
        P("fs", "tp"),
        P("fs", "tp"),
        P(),
        P("fs", "tp"),
        P("fs", "tp"),
        P("fs", "tp"),
    )
    return jax.shard_map(
        body,
        mesh=mesh,
        in_specs=placed,
        out_specs=(
            P(("grp", "tp"), "fs", None),
            P("grp", "fs"),
            P("grp", "fs"),
            P("fs", "grp"),
            P("grp", "fs"),
            P("grp", "fs"),
            P("fs", "grp"),
        ),
        check_vma=False,
    )
```

```python
import jax
import jax.numpy as jnp
from jax import lax
from jax.experimental import pallas as pl
from jax.experimental.pallas import tpu as pltpu
from jax.sharding import PartitionSpec as P

norm_eps = 1e-05
deep_alpha = 2.0**0.25
half_step = 0.5
lane = 128
steps = 4
MESH = pl.DeviceIdType.MESH
ANY = pl.BlockSpec(memory_space=pl.ANY)
VMEM = pl.BlockSpec(memory_space=pltpu.VMEM)


def plain_norm(values):
    row_mean = jnp.mean(values, axis=-1, keepdims=True)
    centred = values - row_mean
    variance = jnp.mean(centred * centred, axis=-1, keepdims=True)
    return centred * lax.rsqrt(variance + norm_eps)


def gated_hidden(inputs, gate_proj, up_proj):
    gate_act = jnp.dot(inputs, gate_proj, preferred_element_type=jnp.float32)
    up_act = jnp.dot(inputs, up_proj, preferred_element_type=jnp.float32)
    return (jax.nn.silu(gate_act) * up_act).astype(jnp.bfloat16)


def relay_weights(gate_proj, up_proj, down_proj):
    gate_rows, up_rows, down_mine = (
        lax.all_gather(gate_proj, "tp", axis=1, tiled=True),
        lax.all_gather(up_proj, "tp", axis=1, tiled=True),
        lax.all_gather(down_proj, "tp", axis=1, tiled=True),
    )
    gate_mine, up_mine = (
        lax.all_to_all(gate_rows, "fs", split_axis=1, concat_axis=0, tiled=True),
        lax.all_to_all(up_rows, "fs", split_axis=1, concat_axis=0, tiled=True),
    )
    return (gate_mine, up_mine, down_mine)


def general_blocks(tokens, norm_gain, first, second):
    fs_index, fs_count = lax.axis_index("fs"), lax.axis_size("fs")
    own_count = tokens.shape[0] // fs_count

    def summed(rows, projs):
        terms = jnp.dot(
            gated_hidden(rows, projs[0], projs[1]), projs[2], preferred_element_type=jnp.float32
        ).astype(jnp.bfloat16)
        parts = lax.all_to_all(
            terms.reshape(fs_count, own_count, -1), "fs", split_axis=0, concat_axis=0
        )
        return jnp.sum(parts.astype(jnp.float32), axis=0)

    own_tokens = lax.dynamic_slice_in_dim(tokens, fs_index * own_count, own_count, 0)
    first = relay_weights(*first)
    second = relay_weights(*second)
    normed_own = plain_norm(
        deep_alpha * own_tokens.astype(jnp.float32) + half_step * summed(tokens, first)
    ).astype(jnp.bfloat16)
    normed = lax.all_gather(normed_own, "fs", axis=0, tiled=True)
    ffn_two = summed(normed, second)
    residual_two = deep_alpha * norm_gain * normed_own.astype(jnp.float32)
    return (plain_norm(residual_two + half_step * ffn_two).astype(jnp.bfloat16), *first, *second)


class Here:
    def __init__(self):
        self.g, self.f, self.t = (lax.axis_index(name) for name in ("grp", "fs", "tp"))
        side = lax.axis_size("tp")
        self.side = side
        self.x, self.c = self.t // 2, self.t % 2
        self.q = self.g * 2 + self.x
        self.xt = (self.t + 2) % side
        self.ct = self.t + 1 - 2 * self.c
        self.xn = (self.g, self.f, self.xt)
        self.yn = (1 - self.g, self.f, self.t)
        self.cn = (self.g, self.f, self.ct)
        last = lax.axis_size("fs") - 1
        self.m = self.f // 2
        self.end = self.f + self.m * (last - 2 * self.f)
        self.inner = (self.g, self.f + 1 - 2 * self.m, self.t)
        self.outer = (self.g, self.f - 1 + 2 * self.m, self.t)
        self.last = last

    def owner(self, mirrored):
        return mirrored + self.m * (self.last - 2 * mirrored)

    def order(self, k):
        f = self.f
        return (f, f + 1 - 2 * (f % 2), (f + 2) % self.side, self.last - f)[k]


def remote(src, dst, send_sem, recv_sem, device):
    return pltpu.make_async_remote_copy(
        src_ref=src,
        dst_ref=dst,
        send_sem=send_sem,
        recv_sem=recv_sem,
        device_id=device,
        device_id_type=MESH,
    )


class PlaneGather:
    kinds = 7

    def __init__(self, here, w, sems, cuts, over_y):
        self.h, self.w, self.sems, self.cuts, self.over_y = here, w, sems, cuts, over_y
        self.rows = w.shape[1] // here.side
        self.quarter = self.rows // 4
        self.piece = self.quarter // cuts
        self.count = cuts * here.side
        self.started = []

    def place(self, p):
        return p // self.h.side, self.h.order(p % self.h.side)

    def region(self, which, cut, z, q):
        first = z * self.rows + q * self.quarter + cut * self.piece
        return self.w.at[which, pl.ds(first, self.piece)]

    def send(self, cut, z, kind, region, device):
        copy = remote(
            region, region, self.sems.at[0, cut, z, kind], self.sems.at[1, cut, z, kind], device
        )
        copy.start()
        self.started.append(copy)

    def arrive(self, cut, z, kind, region):
        remote(
            region, region, self.sems.at[0, cut, z, kind], self.sems.at[1, cut, z, kind], self.h.cn
        ).wait_recv()

    def own(self, p):
        h = self.h
        cut, z = self.place(p)
        region = self.region(h.c, cut, z, h.q)
        self.send(cut, z, 0, region, h.xn)
        self.send(cut, z, 1, region, h.yn)
        self.send(cut, z, 3, region, h.cn)

    def quarters(self):
        h = self.h
        return (h.g * 2 + 1 - h.x, (1 - h.g) * 2 + h.x, (1 - h.g) * 2 + 1 - h.x)

    def forward(self, p):
        h = self.h
        cut, z = self.place(p)
        from_x, from_y, unused = self.quarters()
        region = self.region(h.c, cut, z, from_x)
        self.arrive(cut, z, 0, region)
        if cut < self.over_y:
            self.send(cut, z, 2, region, h.yn)
        self.send(cut, z, 4, region, h.cn)
        region = self.region(h.c, cut, z, from_y)
        self.arrive(cut, z, 1, region)
        if cut >= self.over_y:
            self.send(cut, z, 2, region, h.xn)
        self.send(cut, z, 5, region, h.cn)

    def corner(self, p):
        h = self.h
        cut, z = self.place(p)
        region = self.region(h.c, cut, z, self.quarters()[2])
        self.arrive(cut, z, 2, region)
        self.send(cut, z, 6, region, h.cn)

    def finish(self):
        h, other = self.h, 1 - self.h.c
        from_x, from_y, across = self.quarters()
        for p in range(self.count):
            cut, z = self.place(p)
            for kind, q in ((3, h.q), (4, from_x), (5, from_y), (6, across)):
                self.arrive(cut, z, kind, self.region(other, cut, z, q))

    def drain(self):
        for copy in self.started:
            copy.wait_send()


class DownGather:
    kinds = 5

    def __init__(self, here, src, dst, sems, bounce, local):
        self.h, self.src, self.dst, self.sems = here, src, dst, sems
        self.bounce, self.local = bounce, local
        self.half = src.shape[0] // 2
        self.started = []

    def part(self, g, t):
        return self.dst.at[t, pl.ds(g * self.half, self.half)]

    def send(self, kind, src, dst, device):
        copy = remote(src, dst, self.sems.at[0, kind], self.sems.at[1, kind], device)
        copy.start()
        self.started.append(copy)

    def arrive(self, kind, region):
        remote(
            region, region, self.sems.at[0, kind], self.sems.at[1, kind], self.h.cn
        ).wait_recv()

    def begin(self):
        h = self.h
        self.take = pltpu.make_async_copy(self.src, self.bounce, self.local.at[0])
        self.take.start()
        self.send(
            0, self.src.at[pl.ds(h.g * self.half, self.half)], self.part(h.g, h.t), h.xn
        )
        self.send(2, self.src, self.dst.at[h.t], h.cn)

    def place(self):
        self.take.wait()
        self.put = pltpu.make_async_copy(
            self.bounce, self.dst.at[self.h.t], self.local.at[1]
        )
        self.put.start()

    def forward(self):
        h = self.h
        region = self.part(h.g, h.xt)
        self.arrive(0, region)
        self.send(1, region, region, h.yn)
        self.send(3, region, region, h.cn)

    def corner(self):
        h = self.h
        region = self.part(1 - h.g, h.xt)
        self.arrive(1, region)
        self.send(4, region, region, h.cn)

    def finish(self):
        h = self.h
        across = (h.ct + 2) % h.side
        self.arrive(2, self.dst.at[h.ct])
        self.arrive(3, self.part(h.g, across))
        self.arrive(4, self.part(1 - h.g, across))
        self.put.wait()

    def drain(self):
        for copy in self.started:
            copy.wait_send()


class Placement:
    def __init__(self, here, src, dst, sems, stage, stage_sems, bounce, local, cuts):
        self.h, self.src, self.dst, self.cuts = here, src, dst, cuts
        self.sems, self.stage, self.stage_sems = sems, stage, stage_sems
        self.bounce, self.local = bounce, local
        self.rows = src.shape[1]
        self.quarter = self.rows // 4
        self.piece = self.quarter // cuts

    def target_rows(self, which, cut):
        h = self.h
        first = h.f * self.rows + h.q * self.quarter + cut * self.piece
        return self.dst.at[which, pl.ds(first, self.piece)]

    def direct(self, cut, c):
        h = self.h
        first = h.q * self.quarter + cut * self.piece
        copy = remote(
            self.src.at[c, pl.ds(first, self.piece)],
            self.target_rows(c, cut),
            self.sems.at[0, cut, c],
            self.sems.at[2, cut, h.f],
            (h.g, h.t, 2 * h.x + c),
        )
        return jnp.logical_and(h.f == h.t, h.c == c), copy

    def staged(self, cut):
        h = self.h
        first = (h.g * 2 + 1 - h.x) * self.quarter + cut * self.piece
        return remote(
            self.src.at[:, pl.ds(first, self.piece)],
            self.stage.at[:, pl.ds(cut * self.piece, self.piece)],
            self.stage_sems.at[0, cut],
            self.stage_sems.at[1, cut],
            h.xn,
        )

    def passed_on(self, cut, c):
        h = self.h
        copy = remote(
            self.stage.at[c, pl.ds(cut * self.piece, self.piece)],
            self.target_rows(c, cut),
            self.sems.at[1, cut, c],
            self.sems.at[2, cut, h.f],
            (h.g, h.xt, 2 * h.x + c),
        )
        return jnp.logical_and(h.f == h.xt, h.c == c), copy

    def kept(self, cut):
        h = self.h
        return pltpu.make_async_copy(
            self.stage.at[h.c, pl.ds(cut * self.piece, self.piece)],
            self.target_rows(h.c, cut),
            self.stage_sems.at[2, cut],
        )

    def begin(self):
        for cut in range(self.cuts):
            self.staged(cut).start()
            for c in range(2):
                mine, copy = self.direct(cut, c)

                @pl.when(jnp.logical_not(mine))
                def _():
                    copy.start()

    def local_copy(self):
        h = self.h
        first = h.q * self.quarter

        @pl.when(h.f == h.t)
        def _():
            take = pltpu.make_async_copy(
                self.src.at[h.c, pl.ds(first, self.quarter)], self.bounce, self.local
            )
            take.start()
            take.wait()
            put = pltpu.make_async_copy(
                self.bounce,
                self.dst.at[h.c, pl.ds(h.f * self.rows + first, self.quarter)],
                self.local,
            )
            put.start()
            put.wait()

    def relay(self, cut):
        h = self.h
        self.staged(cut).wait_recv()
        for c in range(2):
            mine, copy = self.passed_on(cut, c)

            @pl.when(jnp.logical_not(mine))
            def _():
                copy.start()

        @pl.when(h.f == h.xt)
        def _():
            self.kept(cut).start()

    def arrived(self, p):
        h = self.h
        cut, k = p // h.side, p % h.side
        z = h.order(k)
        first = z * self.rows + h.q * self.quarter + cut * self.piece
        region = self.dst.at[h.c, pl.ds(first, self.piece)]
        copy = remote(region, region, self.sems.at[0, 0, 0], self.sems.at[2, cut, z], h.cn)
        if k == 0:

            @pl.when(jnp.logical_and(h.f != h.t, h.f != h.xt))
            def _():
                copy.wait_recv()

            @pl.when(h.f == h.xt)
            def _():
                self.kept(cut).wait()

        else:
            copy.wait_recv()

    def finish(self):
        for cut in range(self.cuts):
            self.staged(cut).wait_send()
            for mine, copy in [f(cut, c) for f in (self.direct, self.passed_on) for c in range(2)]:

                @pl.when(jnp.logical_not(mine))
                def _():
                    copy.wait_send()


first_cuts = 4
second_cuts = 2


def weights_kernel(
    src_one, down_src, src_two, w_one, down_one, w_two,
    bounce, down_bounce, stage_one, stage_two, place_sems, stage_sems,
    place_sems_two, stage_sems_two, plane_sems, down_sems, local,
):
    h = Here()
    first = Placement(
        h, src_one, w_one, place_sems, stage_one, stage_sems, bounce, local.at[2], first_cuts
    )
    second = Placement(
        h, src_two, w_two, place_sems_two, stage_two, stage_sems_two, bounce, local.at[2], 1
    )
    gather = PlaneGather(h, w_one, plane_sems, first_cuts, first_cuts // 2)
    down = DownGather(h, down_src, down_one, down_sems, down_bounce, local)
    first.begin()
    down.begin()
    first.local_copy()
    first.relay(0)
    first.relay(1)
    down.place()
    side, count = h.side, gather.count
    for p in range(count + 2 * side):
        if p < count:
            first.arrived(p)
            gather.own(p)
        if 0 < p < first_cuts - 1:
            first.relay(p + 1)
        if p == side:
            down.forward()
        if side <= p < count + side:
            gather.forward(p - side)
        if p >= 2 * side:
            gather.corner(p - 2 * side)
        if p == side + 2:
            second.begin()
        if p == 3 * side:
            down.corner()
            second.relay(0)
    second.local_copy()
    gather.finish()
    down.finish()
    for p in range(side):
        second.arrived(p)
    gather.drain()
    down.drain()
    first.finish()
    second.finish()


def gather_weights(src_one, down_src, src_two):
    side = lax.axis_size("tp")
    two, rows, width = src_one.shape
    full = jax.ShapeDtypeStruct((two, rows * side, width), src_one.dtype)
    down = jax.ShapeDtypeStruct((side, *down_src.shape), down_src.dtype)
    return pl.pallas_call(
        weights_kernel,
        out_shape=(full, down, full),
        in_specs=[ANY] * 3,
        out_specs=(ANY,) * 3,
        scratch_shapes=[
            pltpu.VMEM((rows // 4, width), src_one.dtype),
            pltpu.VMEM(down_src.shape, down_src.dtype),
            pltpu.VMEM((two, rows // 4, width), src_one.dtype),
            pltpu.VMEM((two, rows // 4, width), src_one.dtype),
            pltpu.SemaphoreType.DMA((3, first_cuts, side)),
            pltpu.SemaphoreType.DMA((3, first_cuts)),
            pltpu.SemaphoreType.DMA((3, 1, side)),
            pltpu.SemaphoreType.DMA((3, 1)),
            pltpu.SemaphoreType.DMA((2, first_cuts, side, PlaneGather.kinds)),
            pltpu.SemaphoreType.DMA((2, DownGather.kinds)),
            pltpu.SemaphoreType.DMA((3,)),
        ],
        compiler_params=pltpu.CompilerParams(has_side_effects=True),
        name="gather_weights",
    )(src_one, down_src, src_two)


def gate_part(rows, w_in, j, hidden):
    act = jnp.dot(rows, w_in[j], preferred_element_type=jnp.float32)
    gate_act, up_act = act[:, :lane], act[:, lane:]
    value = gate_act / (1.0 + jnp.exp(-gate_act)) * up_act
    hidden[:, pl.ds(pl.multiple_of(j * lane, lane), lane)] = value.astype(jnp.bfloat16)


def compute_kernel(
    tokens, w, down, terms, gate_out, up_out, down_out,
    rows_in, w_in, down_in, hidden, terms_in, sems,
):
    groups = w.shape[2] // lane
    wide = 4 * lane
    spans = down_out.shape[1] // wide
    parts, unused, cols = down.shape

    def w_load(which, j):
        return pltpu.make_async_copy(
            w.at[which, :, pl.ds(pl.multiple_of(j * lane, lane), lane)],
            w_in.at[j, :, pl.ds(which * lane, lane)],
            sems.at[which, j],
        )

    def w_store(which, j):
        return pltpu.make_async_copy(
            w_in.at[j, :, pl.ds(which * lane, lane)],
            (gate_out, up_out)[which].at[:, pl.ds(pl.multiple_of(j * lane, lane), lane)],
            sems.at[2 + which, j],
        )

    take_rows = pltpu.make_async_copy(tokens, rows_in, sems.at[4, 0])
    take_down = [
        pltpu.make_async_copy(
            down.at[i], down_in.at[:, pl.ds(i * cols, cols)], sems.at[4, 3 + i]
        )
        for i in range(parts)
    ]
    give_down = pltpu.make_async_copy(down_in, down_out, sems.at[4, 1])
    take_rows.start()

    @pl.loop(0, groups)
    def _(j):
        w_load(0, j).start()
        w_load(1, j).start()

    for copy in take_down:
        copy.start()
    take_rows.wait()

    @pl.loop(0, groups)
    def _(j):
        w_load(0, j).wait()
        w_load(1, j).wait()
        w_store(0, j).start()
        w_store(1, j).start()

        gate_part(rows_in[...], w_in, j, hidden)

    for copy in take_down:
        copy.wait()
    give_down.start()

    @pl.loop(0, spans)
    def _(n):
        cols = pl.ds(pl.multiple_of(n * wide, wide), wide)

        terms_in[:, cols] = jnp.dot(
            hidden[...], down_in[:, cols], preferred_element_type=jnp.float32
        ).astype(jnp.bfloat16)

    give_terms = pltpu.make_async_copy(terms_in, terms, sems.at[4, 2])
    give_terms.start()

    @pl.loop(0, groups)
    def _(j):
        w_store(0, j).wait()
        w_store(1, j).wait()

    give_down.wait()
    give_terms.wait()


def compute_terms(tokens, w, down):
    two, depth, width = w.shape
    count = tokens.shape[0]
    groups = width // lane
    parts, down_rows, cols = down.shape
    down_shape = (down_rows, parts * cols)
    proj = jax.ShapeDtypeStruct((depth, width), w.dtype)
    flops = 2 * count * depth * width * 3
    return pl.pallas_call(
        compute_kernel,
        out_shape=(
            jax.ShapeDtypeStruct((count, parts * cols), jnp.bfloat16),
            proj,
            proj,
            jax.ShapeDtypeStruct(down_shape, down.dtype),
        ),
        in_specs=[ANY] * 3,
        out_specs=(ANY,) * 4,
        scratch_shapes=[
            pltpu.VMEM(tokens.shape, tokens.dtype),
            pltpu.VMEM((groups, depth, 2 * lane), w.dtype),
            pltpu.VMEM(down_shape, down.dtype),
            pltpu.VMEM((count, width), jnp.bfloat16),
            pltpu.VMEM((count, parts * cols), jnp.bfloat16),
            pltpu.SemaphoreType.DMA((5, max(groups, 3 + parts))),
        ],
        compiler_params=pltpu.CompilerParams(vmem_limit_bytes=56 * 1024 * 1024),
        cost_estimate=pl.CostEstimate(flops=flops, bytes_accessed=6 * w.size, transcendentals=0),
        name="compute_terms",
    )(tokens, w, down)


class LineSum:
    kinds = 6

    def __init__(self, here, terms, place, from_outer, from_inner, from_middle, to_inner, to_outer, sems):
        self.h, self.terms, self.place = here, terms, place
        self.from_outer, self.from_inner, self.from_middle = from_outer, from_inner, from_middle
        self.to_inner, self.to_outer, self.sems = to_inner, to_outer, sems
        self.own = terms.shape[0] // (here.last + 1)
        self.size = self.own // steps

    def term(self, mirrored, s):
        return self.place(self.h.owner(mirrored), s)

    def at(self, s):
        return pl.ds(pl.multiple_of(s * self.size, self.size), self.size)

    def copy(self, src, dst, kind, s, device):
        return remote(src, dst, self.sems.at[0, kind, s], self.sems.at[1, kind, s], device)

    def start_copy(self, o, s):
        slot = 3 - o
        return self.copy(
            self.terms.at[self.term(o, s)], self.from_outer.at[slot, self.at(s)], slot, s,
            self.h.inner,
        )

    def middle_copy(self, o, s):
        slot = 3 - o
        return self.copy(
            self.to_inner.at[slot, self.at(s)], self.from_middle.at[slot, self.at(s)], 3 + slot,
            s, self.h.inner,
        )

    def back_copy(self, s):
        return self.copy(
            self.to_outer.at[self.at(s)], self.from_inner.at[self.at(s)], 5, s, self.h.outer
        )

    def send_start(self, s):
        for o in (3, 2, 1):
            self.start_copy(o, s).start()

    def relay(self, s):
        at = self.at(s)
        for o in (3, 2):
            slot = 3 - o
            self.start_copy(o, s).wait_recv()
            self.to_inner[slot, at, :] = (
                self.from_outer[slot, at, :].astype(jnp.float32)
                + self.terms[self.term(o, s), :].astype(jnp.float32)
            ).astype(jnp.bfloat16)
            self.middle_copy(o, s).start()

    def relay_back(self, s):
        at = self.at(s)
        self.middle_copy(3, s).wait_recv()
        self.to_outer[at, :] = (
            self.from_middle[0, at, :].astype(jnp.float32)
            + self.terms[self.term(0, s), :].astype(jnp.float32)
        ).astype(jnp.bfloat16)
        self.back_copy(s).start()

    def inner_total(self, s):
        at = self.at(s)
        self.start_copy(1, s).wait_recv()
        self.middle_copy(2, s).wait_recv()
        return (
            self.from_outer[2, at, :].astype(jnp.float32)
            + self.terms[self.term(1, s), :].astype(jnp.float32)
        ) + self.from_middle[1, at, :].astype(jnp.float32)

    def end_total(self, s):
        at = self.at(s)
        self.back_copy(s).wait_recv()
        return self.terms[self.term(0, s), :].astype(jnp.float32) + self.from_inner[
            at, :
        ].astype(jnp.float32)

    def finish_end(self, s):
        for o in (3, 2, 1):
            self.start_copy(o, s).wait_send()

    def finish_inner(self, s):
        self.middle_copy(3, s).wait_send()
        self.middle_copy(2, s).wait_send()
        self.back_copy(s).wait_send()


def line_scratch(own, width):
    def rows(*lead):
        return pltpu.VMEM((*lead, own, width), jnp.bfloat16)

    return [
        rows(3), rows(), rows(2), rows(2), rows(),
        pltpu.SemaphoreType.DMA((2, LineSum.kinds, steps)),
    ]


class LineSpread:
    kinds = 6

    def __init__(self, here, out, place, sems):
        self.h, self.out, self.place, self.sems = here, out, place, sems

    def copy(self, mirrored, kind, s, device):
        rows = self.out.at[self.place(self.h.owner(mirrored), s)]
        return remote(
            rows, rows, self.sems.at[0, kind, s], self.sems.at[1, kind, s], device
        )

    def in_zero(self, s):
        return self.copy(0, 0, s, self.h.inner)

    def cross_one(self, s):
        return self.copy(1, 1, s, self.h.inner)

    def cross_zero(self, s):
        return self.copy(0, 2, s, self.h.inner)

    def out_any(self, o, s):
        return self.copy(o, 2 + o, s, self.h.outer)

    def hand_on(self, s):
        self.in_zero(s).wait_recv()
        self.cross_zero(s).start()
        self.copy(2, 1, s, self.h.inner).wait_recv()
        self.out_any(2, s).start()
        self.copy(3, 2, s, self.h.inner).wait_recv()
        self.out_any(3, s).start()

    def finish_inner(self, s):
        self.cross_one(s).wait_send()
        self.cross_zero(s).wait_send()
        for o in (1, 2, 3):
            self.out_any(o, s).wait_send()


halves = 2


def blocks_kernel(
    terms_one, tokens, gain, w_in, down_src, result, w, down,
    own_rows, normed, terms_two, hidden, w_held, down_held, down_bounce,
    outer_one, inner_one, middle_one, to_inner_one, to_outer_one, line_one,
    outer_two, inner_two, middle_two, to_inner_two, to_outer_two, line_two,
    spread_sems, plane_sems, down_sems, local, load_sems,
):
    h = Here()
    own, size = result.shape[0], result.shape[0] // steps
    count = normed.shape[0]
    half, per = count // halves, steps // halves
    is_end, is_inner = h.end == 0, h.end == 1

    def span(first, length):
        return pl.ds(pl.multiple_of(first, size), length)

    def plain_place(owner, s):
        return span(owner * own + s * size, size)

    def half_place(owner, s):
        return span((s // per) * half + owner * (own // halves) + (s % per) * size, size)

    one = LineSum(
        h, terms_one, plain_place, outer_one, inner_one, middle_one, to_inner_one, to_outer_one,
        line_one,
    )
    two = LineSum(
        h, terms_two, half_place, outer_two, inner_two, middle_two, to_inner_two, to_outer_two,
        line_two,
    )
    spread = LineSpread(h, normed, half_place, spread_sems)
    gather = PlaneGather(h, w, plane_sems, second_cuts, 1)
    down_part = DownGather(h, down_src, down, down_sems, down_bounce, local)
    take = pltpu.make_async_copy(tokens.at[span(h.f * own, own)], own_rows, local.at[2])
    take.start()

    @pl.when(is_end)
    def _():
        one.send_start(0)

    for p in range(gather.count):
        gather.own(p)
    down_part.begin()
    down_part.place()
    take.wait()

    def keep_one(s, total):
        at = pl.ds(s * size, size)
        normed[half_place(h.f, s), :] = plain_norm(
            deep_alpha * own_rows[at, :].astype(jnp.float32) + half_step * total
        ).astype(jnp.bfloat16)

    def keep_two(s, total):
        residual = deep_alpha * gain[...] * normed[half_place(h.f, s), :].astype(jnp.float32)
        result[pl.ds(s * size, size), :] = plain_norm(residual + half_step * total).astype(
            jnp.bfloat16
        )

    groups = w.shape[2] // lane
    wide = 4 * lane

    def w_load(which, j):
        return pltpu.make_async_copy(
            w.at[which, :, pl.ds(pl.multiple_of(j * lane, lane), lane)],
            w_held.at[j, :, pl.ds(which * lane, lane)],
            load_sems.at[which, j],
        )

    cols = down.shape[2]
    down_load = [
        pltpu.make_async_copy(
            down.at[i], down_held.at[:, pl.ds(i * cols, cols)], local.at[3 + i]
        )
        for i in range(h.side)
    ]

    def load():
        gather.finish()
        down_part.finish()

        @pl.loop(0, groups)
        def _(j):
            w_load(0, j).start()
            w_load(1, j).start()

        for copy in down_load:
            copy.start()

    def hide(part, first, last, wait=False):
        rows = normed.at[pl.ds(part * half, half)]

        @pl.loop(first, last)
        def _(j):
            if wait:
                w_load(0, j).wait()
                w_load(1, j).wait()
            gate_part(rows[...], w_held, j, hidden)

    def sink(part):
        @pl.loop(0, down_held.shape[1] // wide)
        def _(n):
            cols = pl.ds(pl.multiple_of(n * wide, wide), wide)
            terms_two[pl.ds(part * half, half), cols] = jnp.dot(
                hidden[...], down_held[:, cols], preferred_element_type=jnp.float32
            ).astype(jnp.bfloat16)

    def spread_end(first, last):
        @pl.when(is_end)
        def _():
            for s in range(first, last):
                for o in (1, 2, 3):
                    spread.out_any(o, s).wait_recv()

    def send_two(first, last):
        @pl.when(is_end)
        def _():
            for s in range(first, last):
                two.send_start(s)

    def relay_two(s):
        @pl.when(is_inner)
        def _():
            two.relay(s)
            two.relay_back(s)
            keep_two(s, two.inner_total(s))

    def forward(first, last):
        return [lambda p=p: gather.forward(p) for p in range(first, last)]

    def corner(first, last):
        return [lambda p=p: gather.corner(p) for p in range(first, last)]

    cut = (groups + 1) // 2
    jobs = {
        1: forward(0, 6),
        2: [*forward(6, 8), *corner(0, 4), down_part.forward],
        3: [
            *corner(4, 8),
            down_part.corner,
            load,
            lambda: spread_end(0, per),
            lambda: hide(0, 0, cut, True),
        ],
    }
    for s in range(steps):

        @pl.when(is_inner)
        def _():
            one.relay(s)
            one.relay_back(s)
            keep_one(s, one.inner_total(s))
            spread.cross_one(s).start()
            spread.out_any(1, s).start()
            if s >= 1:
                spread.hand_on(s - 1)

        @pl.when(is_end)
        def _():
            if s + 1 < steps:
                one.send_start(s + 1)
            keep_one(s, one.end_total(s))
            spread.in_zero(s).start()

        for job in jobs.get(s, ()):
            job()

    @pl.when(is_inner)
    def _():
        spread.hand_on(steps - 1)

    hide(0, cut, groups, True)
    for copy in down_load:
        copy.wait()
    sink(0)
    send_two(0, per)
    spread_end(per, steps)
    hide(1, 0, cut)
    relay_two(0)
    hide(1, cut, groups)
    relay_two(1)
    sink(1)
    send_two(per, steps)
    for s in range(2, steps):
        relay_two(s)

    @pl.when(is_end)
    def _():
        for s in range(steps):
            keep_two(s, two.end_total(s))

    gather.drain()
    down_part.drain()
    for s in range(steps):

        @pl.when(is_end)
        def _():
            one.finish_end(s)
            two.finish_end(s)
            spread.in_zero(s).wait_send()

        @pl.when(is_inner)
        def _():
            one.finish_inner(s)
            two.finish_inner(s)
            spread.finish_inner(s)


def blocks(terms, tokens, gain, w, down_src):
    side = lax.axis_size("tp")
    count, width = terms.shape
    own = count // lax.axis_size("fs")
    two, depth, hidden = w.shape
    groups = hidden // lane
    down_rows, cols = down_src.shape
    return pl.pallas_call(
        blocks_kernel,
        out_shape=(
            jax.ShapeDtypeStruct((own, width), jnp.bfloat16),
            jax.ShapeDtypeStruct(w.shape, w.dtype),
            jax.ShapeDtypeStruct((side, down_rows, cols), down_src.dtype),
        ),
        in_specs=[VMEM, ANY, VMEM, ANY, ANY],
        out_specs=(VMEM, ANY, ANY),
        input_output_aliases={3: 1},
        scratch_shapes=[
            pltpu.VMEM((own, width), jnp.bfloat16),
            pltpu.VMEM((count, width), jnp.bfloat16),
            pltpu.VMEM((count, width), jnp.bfloat16),
            pltpu.VMEM((count // halves, hidden), jnp.bfloat16),
            pltpu.VMEM((groups, depth, two * lane), w.dtype),
            pltpu.VMEM((down_rows, side * cols), down_src.dtype),
            pltpu.VMEM(down_src.shape, down_src.dtype),
            *line_scratch(own, width),
            *line_scratch(own, width),
            pltpu.SemaphoreType.DMA((2, LineSpread.kinds, steps)),
            pltpu.SemaphoreType.DMA((2, second_cuts, side, PlaneGather.kinds)),
            pltpu.SemaphoreType.DMA((2, DownGather.kinds)),
            pltpu.SemaphoreType.DMA((3 + side,)),
            pltpu.SemaphoreType.DMA((2, groups)),
        ],
        compiler_params=pltpu.CompilerParams(
            has_side_effects=True, vmem_limit_bytes=63 * 1024 * 1024
        ),
        name="sum_norm_blocks",
    )(terms, tokens, gain, w, down_src)


emit_cuts = 8


def emit_kernel(w, down, gate_out, up_out, down_out, w_held, down_held, sems):
    rows = w.shape[1] // emit_cuts
    parts, unused, cols = down.shape
    moves = []
    for i in range(parts):
        at = pl.ds(i * cols, cols)
        moves.append((down.at[i], down_held.at[:, at], down_out.at[:, at]))
    for i in range(emit_cuts):
        at = pl.ds(i * rows, rows)
        for which, out in enumerate((gate_out, up_out)):
            moves.append((w.at[which, at], w_held.at[which, at], out.at[at]))
    takes = [pltpu.make_async_copy(m[0], m[1], sems.at[0, i]) for i, m in enumerate(moves)]
    gives = [pltpu.make_async_copy(m[1], m[2], sems.at[1, i]) for i, m in enumerate(moves)]
    for take in takes:
        take.start()
    for take, give in zip(takes, gives):
        take.wait()
        give.start()
    for give in gives:
        give.wait()


def emit(w, down):
    two, depth, width = w.shape
    parts, down_rows, cols = down.shape
    proj = jax.ShapeDtypeStruct((depth, width), w.dtype)
    down_shape = (down_rows, parts * cols)
    return pl.pallas_call(
        emit_kernel,
        out_shape=(proj, proj, jax.ShapeDtypeStruct(down_shape, down.dtype)),
        in_specs=[ANY] * 2,
        out_specs=(ANY,) * 3,
        scratch_shapes=[
            pltpu.VMEM(w.shape, w.dtype),
            pltpu.VMEM(down_shape, down.dtype),
            pltpu.SemaphoreType.DMA((2, two * emit_cuts + parts)),
        ],
        compiler_params=pltpu.CompilerParams(vmem_limit_bytes=56 * 1024 * 1024),
        name="emit_projections",
    )(w, down)


def body(prompt, gate_first, up_first, down_first, norm_gain, gate_second, up_second, down_second):
    side, groups, planes = lax.axis_size("tp"), lax.axis_size("grp"), lax.axis_size("fs")
    fs_index = lax.axis_index("fs")
    tokens = prompt.reshape(-1, prompt.shape[-1])
    row_block, width = gate_first.shape
    gain_rows = lax.dynamic_slice_in_dim(norm_gain, fs_index * row_block, row_block, 0)[:, None]
    down_a, down_b = down_first.astype(jnp.bfloat16), down_second.astype(jnp.bfloat16)
    planar = (
        groups == 2
        and side == 2 * groups
        and planes == side
        and row_block % (4 * 64) == 0
        and width % lane == 0
        and down_first.shape[0] % 32 == 0
        and down_first.shape[1] % lane == 0
        and tokens.shape[0] % (planes * steps * 16) == 0
        and tokens.shape[0] % (halves * planes * 16) == 0
        and tokens.shape[1] % (4 * lane) == 0
    )
    if planar:
        src_one = jnp.stack([gate_first.astype(jnp.bfloat16), up_first.astype(jnp.bfloat16)])
        src_two = jnp.stack(
            [
                (gain_rows * gate_second).astype(jnp.bfloat16),
                (gain_rows * up_second).astype(jnp.bfloat16),
            ]
        )
        w_one, down_one, w_two = gather_weights(src_one, down_a, src_two)
        terms_one, gate_one, up_one, down_one = compute_terms(tokens, w_one, down_one)
        result, w_two, down_two = blocks(terms_one, tokens, norm_gain[None, :], w_two, down_b)
        gate_two, up_two, down_two = emit(w_two, down_two)
    else:
        result, gate_one, up_one, down_one, gate_two, up_two, down_two = general_blocks(
            tokens,
            norm_gain,
            (gate_first.astype(jnp.bfloat16), up_first.astype(jnp.bfloat16), down_a),
            (
                (gain_rows * gate_second).astype(jnp.bfloat16),
                (gain_rows * up_second).astype(jnp.bfloat16),
                down_b,
            ),
        )
    return (
        result.reshape(1, result.shape[0], result.shape[-1]),
        gate_one,
        up_one,
        down_one,
        gate_two,
        up_two,
        down_two,
    )


def solution(mesh):
    placed = (
        P(("grp", "tp"), None, None),
        P("fs", "tp"),
        P("fs", "tp"),
        P("fs", "tp"),
        P(),
        P("fs", "tp"),
        P("fs", "tp"),
        P("fs", "tp"),
    )
    return jax.shard_map(
        body,
        mesh=mesh,
        in_specs=placed,
        out_specs=(
            P(("grp", "tp"), "fs", None),
            P("grp", "fs"),
            P("grp", "fs"),
            P("fs", "grp"),
            P("grp", "fs"),
            P("grp", "fs"),
            P("fs", "grp"),
        ),
        check_vma=False,
    )
```

```python
import jax
import jax.numpy as jnp
from jax import lax
from jax.experimental import pallas as pl
from jax.experimental.pallas import tpu as pltpu
from jax.sharding import PartitionSpec as P

norm_eps = 1e-05
deep_alpha = 2.0**0.25
half_step = 0.5
lane = 128
steps = 4
MESH = pl.DeviceIdType.MESH
ANY = pl.BlockSpec(memory_space=pl.ANY)
VMEM = pl.BlockSpec(memory_space=pltpu.VMEM)


def plain_norm(values):
    row_mean = jnp.mean(values, axis=-1, keepdims=True)
    centred = values - row_mean
    variance = jnp.mean(centred * centred, axis=-1, keepdims=True)
    return centred * lax.rsqrt(variance + norm_eps)


def gated_hidden(inputs, gate_proj, up_proj):
    gate_act = jnp.dot(inputs, gate_proj, preferred_element_type=jnp.float32)
    up_act = jnp.dot(inputs, up_proj, preferred_element_type=jnp.float32)
    return (jax.nn.silu(gate_act) * up_act).astype(jnp.bfloat16)


def relay_weights(gate_proj, up_proj, down_proj):
    gate_rows, up_rows, down_mine = (
        lax.all_gather(gate_proj, "tp", axis=1, tiled=True),
        lax.all_gather(up_proj, "tp", axis=1, tiled=True),
        lax.all_gather(down_proj, "tp", axis=1, tiled=True),
    )
    gate_mine, up_mine = (
        lax.all_to_all(gate_rows, "fs", split_axis=1, concat_axis=0, tiled=True),
        lax.all_to_all(up_rows, "fs", split_axis=1, concat_axis=0, tiled=True),
    )
    return (gate_mine, up_mine, down_mine)


def general_blocks(tokens, norm_gain, first, second):
    fs_index, fs_count = lax.axis_index("fs"), lax.axis_size("fs")
    own_count = tokens.shape[0] // fs_count

    def summed(rows, projs):
        terms = jnp.dot(
            gated_hidden(rows, projs[0], projs[1]), projs[2], preferred_element_type=jnp.float32
        ).astype(jnp.bfloat16)
        parts = lax.all_to_all(
            terms.reshape(fs_count, own_count, -1), "fs", split_axis=0, concat_axis=0
        )
        return jnp.sum(parts.astype(jnp.float32), axis=0)

    own_tokens = lax.dynamic_slice_in_dim(tokens, fs_index * own_count, own_count, 0)
    first = relay_weights(*first)
    second = relay_weights(*second)
    normed_own = plain_norm(
        deep_alpha * own_tokens.astype(jnp.float32) + half_step * summed(tokens, first)
    ).astype(jnp.bfloat16)
    normed = lax.all_gather(normed_own, "fs", axis=0, tiled=True)
    ffn_two = summed(normed, second)
    residual_two = deep_alpha * norm_gain * normed_own.astype(jnp.float32)
    return (plain_norm(residual_two + half_step * ffn_two).astype(jnp.bfloat16), *first, *second)


class Here:
    def __init__(self):
        self.g, self.f, self.t = (lax.axis_index(name) for name in ("grp", "fs", "tp"))
        side = lax.axis_size("tp")
        self.side = side
        self.x, self.c = self.t // 2, self.t % 2
        self.q = self.g * 2 + self.x
        self.xt = (self.t + 2) % side
        self.ct = self.t + 1 - 2 * self.c
        self.xn = (self.g, self.f, self.xt)
        self.yn = (1 - self.g, self.f, self.t)
        self.cn = (self.g, self.f, self.ct)
        last = lax.axis_size("fs") - 1
        self.m = self.f // 2
        self.end = self.f + self.m * (last - 2 * self.f)
        self.inner = (self.g, self.f + 1 - 2 * self.m, self.t)
        self.outer = (self.g, self.f - 1 + 2 * self.m, self.t)
        self.last = last

    def owner(self, mirrored):
        return mirrored + self.m * (self.last - 2 * mirrored)

    def order(self, k):
        f = self.f
        return (f, f + 1 - 2 * (f % 2), (f + 2) % self.side, self.last - f)[k]


def remote(src, dst, send_sem, recv_sem, device):
    return pltpu.make_async_remote_copy(
        src_ref=src,
        dst_ref=dst,
        send_sem=send_sem,
        recv_sem=recv_sem,
        device_id=device,
        device_id_type=MESH,
    )


class PlaneGather:
    kinds = 7

    def __init__(self, here, w, sems, cuts, over_y):
        self.h, self.w, self.sems, self.cuts, self.over_y = here, w, sems, cuts, over_y
        self.rows = w.shape[1] // here.side
        self.quarter = self.rows // 4
        self.piece = self.quarter // cuts
        self.count = cuts * here.side
        self.started = []

    def place(self, p):
        return p // self.h.side, self.h.order(p % self.h.side)

    def region(self, which, cut, z, q):
        first = z * self.rows + q * self.quarter + cut * self.piece
        return self.w.at[which, pl.ds(first, self.piece)]

    def send(self, cut, z, kind, region, device):
        copy = remote(
            region, region, self.sems.at[0, cut, z, kind], self.sems.at[1, cut, z, kind], device
        )
        copy.start()
        self.started.append(copy)

    def arrive(self, cut, z, kind, region):
        remote(
            region, region, self.sems.at[0, cut, z, kind], self.sems.at[1, cut, z, kind], self.h.cn
        ).wait_recv()

    def own(self, p):
        h = self.h
        cut, z = self.place(p)
        region = self.region(h.c, cut, z, h.q)
        self.send(cut, z, 0, region, h.xn)
        self.send(cut, z, 1, region, h.yn)
        self.send(cut, z, 3, region, h.cn)

    def quarters(self):
        h = self.h
        return (h.g * 2 + 1 - h.x, (1 - h.g) * 2 + h.x, (1 - h.g) * 2 + 1 - h.x)

    def forward(self, p):
        h = self.h
        cut, z = self.place(p)
        from_x, from_y, unused = self.quarters()
        region = self.region(h.c, cut, z, from_x)
        self.arrive(cut, z, 0, region)
        if cut < self.over_y:
            self.send(cut, z, 2, region, h.yn)
        self.send(cut, z, 4, region, h.cn)
        region = self.region(h.c, cut, z, from_y)
        self.arrive(cut, z, 1, region)
        if cut >= self.over_y:
            self.send(cut, z, 2, region, h.xn)
        self.send(cut, z, 5, region, h.cn)

    def corner(self, p):
        h = self.h
        cut, z = self.place(p)
        region = self.region(h.c, cut, z, self.quarters()[2])
        self.arrive(cut, z, 2, region)
        self.send(cut, z, 6, region, h.cn)

    def finish(self):
        h, other = self.h, 1 - self.h.c
        from_x, from_y, across = self.quarters()
        for p in range(self.count):
            cut, z = self.place(p)
            for kind, q in ((3, h.q), (4, from_x), (5, from_y), (6, across)):
                self.arrive(cut, z, kind, self.region(other, cut, z, q))

    def drain(self):
        for copy in self.started:
            copy.wait_send()


class DownGather:
    kinds = 5

    def __init__(self, here, src, dst, sems, bounce, local):
        self.h, self.src, self.dst, self.sems = here, src, dst, sems
        self.bounce, self.local = bounce, local
        self.half = src.shape[0] // 2
        self.started = []

    def part(self, g, t):
        return self.dst.at[t, pl.ds(g * self.half, self.half)]

    def send(self, kind, src, dst, device):
        copy = remote(src, dst, self.sems.at[0, kind], self.sems.at[1, kind], device)
        copy.start()
        self.started.append(copy)

    def arrive(self, kind, region):
        remote(
            region, region, self.sems.at[0, kind], self.sems.at[1, kind], self.h.cn
        ).wait_recv()

    def begin(self):
        h = self.h
        self.take = pltpu.make_async_copy(self.src, self.bounce, self.local.at[0])
        self.take.start()
        self.send(
            0, self.src.at[pl.ds(h.g * self.half, self.half)], self.part(h.g, h.t), h.xn
        )
        self.send(2, self.src, self.dst.at[h.t], h.cn)

    def place(self):
        self.take.wait()
        self.put = pltpu.make_async_copy(
            self.bounce, self.dst.at[self.h.t], self.local.at[1]
        )
        self.put.start()

    def forward(self):
        h = self.h
        region = self.part(h.g, h.xt)
        self.arrive(0, region)
        self.send(1, region, region, h.yn)
        self.send(3, region, region, h.cn)

    def corner(self):
        h = self.h
        region = self.part(1 - h.g, h.xt)
        self.arrive(1, region)
        self.send(4, region, region, h.cn)

    def finish(self):
        h = self.h
        across = (h.ct + 2) % h.side
        self.arrive(2, self.dst.at[h.ct])
        self.arrive(3, self.part(h.g, across))
        self.arrive(4, self.part(1 - h.g, across))
        self.put.wait()

    def drain(self):
        for copy in self.started:
            copy.wait_send()


class Placement:
    def __init__(self, here, src, dst, sems, stage, stage_sems, bounce, local, cuts):
        self.h, self.src, self.dst, self.cuts = here, src, dst, cuts
        self.sems, self.stage, self.stage_sems = sems, stage, stage_sems
        self.bounce, self.local = bounce, local
        self.rows = src.shape[1]
        self.quarter = self.rows // 4
        self.piece = self.quarter // cuts

    def target_rows(self, which, cut):
        h = self.h
        first = h.f * self.rows + h.q * self.quarter + cut * self.piece
        return self.dst.at[which, pl.ds(first, self.piece)]

    def direct(self, cut, c):
        h = self.h
        first = h.q * self.quarter + cut * self.piece
        copy = remote(
            self.src.at[c, pl.ds(first, self.piece)],
            self.target_rows(c, cut),
            self.sems.at[0, cut, c],
            self.sems.at[2, cut, h.f],
            (h.g, h.t, 2 * h.x + c),
        )
        return jnp.logical_and(h.f == h.t, h.c == c), copy

    def staged(self, cut):
        h = self.h
        first = (h.g * 2 + 1 - h.x) * self.quarter + cut * self.piece
        return remote(
            self.src.at[:, pl.ds(first, self.piece)],
            self.stage.at[:, pl.ds(cut * self.piece, self.piece)],
            self.stage_sems.at[0, cut],
            self.stage_sems.at[1, cut],
            h.xn,
        )

    def passed_on(self, cut, c):
        h = self.h
        copy = remote(
            self.stage.at[c, pl.ds(cut * self.piece, self.piece)],
            self.target_rows(c, cut),
            self.sems.at[1, cut, c],
            self.sems.at[2, cut, h.f],
            (h.g, h.xt, 2 * h.x + c),
        )
        return jnp.logical_and(h.f == h.xt, h.c == c), copy

    def kept(self, cut):
        h = self.h
        return pltpu.make_async_copy(
            self.stage.at[h.c, pl.ds(cut * self.piece, self.piece)],
            self.target_rows(h.c, cut),
            self.stage_sems.at[2, cut],
        )

    def begin(self):
        for cut in range(self.cuts):
            self.staged(cut).start()
            for c in range(2):
                mine, copy = self.direct(cut, c)

                @pl.when(jnp.logical_not(mine))
                def _():
                    copy.start()

    def local_copy(self):
        h = self.h
        first = h.q * self.quarter

        @pl.when(h.f == h.t)
        def _():
            held = self.src.at[h.c, pl.ds(first, self.quarter)]
            if self.bounce is not None:
                take = pltpu.make_async_copy(held, self.bounce, self.local)
                take.start()
                take.wait()
                held = self.bounce
            put = pltpu.make_async_copy(
                held,
                self.dst.at[h.c, pl.ds(h.f * self.rows + first, self.quarter)],
                self.local,
            )
            put.start()
            put.wait()

    def relay(self, cut):
        h = self.h
        self.staged(cut).wait_recv()
        for c in range(2):
            mine, copy = self.passed_on(cut, c)

            @pl.when(jnp.logical_not(mine))
            def _():
                copy.start()

        @pl.when(h.f == h.xt)
        def _():
            self.kept(cut).start()

    def arrived(self, p):
        h = self.h
        cut, k = p // h.side, p % h.side
        z = h.order(k)
        first = z * self.rows + h.q * self.quarter + cut * self.piece
        region = self.dst.at[h.c, pl.ds(first, self.piece)]
        copy = remote(region, region, self.sems.at[0, 0, 0], self.sems.at[2, cut, z], h.cn)
        if k == 0:

            @pl.when(jnp.logical_and(h.f != h.t, h.f != h.xt))
            def _():
                copy.wait_recv()

            @pl.when(h.f == h.xt)
            def _():
                self.kept(cut).wait()

        else:
            copy.wait_recv()

    def finish(self):
        for cut in range(self.cuts):
            self.staged(cut).wait_send()
            for mine, copy in [f(cut, c) for f in (self.direct, self.passed_on) for c in range(2)]:

                @pl.when(jnp.logical_not(mine))
                def _():
                    copy.wait_send()


first_cuts = 4
second_cuts = 2


def weights_kernel(
    src_one, down_src, gate_two, up_two, gain, w_one, down_one, w_two,
    raw_two, src_two, bounce, down_bounce, stage_one, stage_two, place_sems, stage_sems,
    place_sems_two, stage_sems_two, plane_sems, down_sems, local,
):
    h = Here()
    first = Placement(
        h, src_one, w_one, place_sems, stage_one, stage_sems, bounce, local.at[2], first_cuts
    )
    second = Placement(
        h, src_two, w_two, place_sems_two, stage_two, stage_sems_two, None, local.at[2], 1
    )
    gather = PlaneGather(h, w_one, plane_sems, first_cuts, first_cuts // 2)
    down = DownGather(h, down_src, down_one, down_sems, down_bounce, local)
    takes = [
        pltpu.make_async_copy(proj, raw_two.at[i], local.at[3 + i])
        for i, proj in enumerate((gate_two, up_two))
    ]
    first.begin()
    down.begin()
    for copy in takes:
        copy.start()
    first.local_copy()
    first.relay(0)
    first.relay(1)
    down.place()
    for copy in takes:
        copy.wait()
    block = lane // 2

    @pl.loop(0, src_two.shape[1] // block)
    def _(i):
        at = pl.ds(pl.multiple_of(i * block, block), block)
        for which in range(2):
            src_two[which, at, :] = (gain[at, :] * raw_two[which, at, :]).astype(jnp.bfloat16)

    side, count = h.side, gather.count
    for p in range(count + 2 * side):
        if p < count:
            first.arrived(p)
            gather.own(p)
        if 0 < p < first_cuts - 1:
            first.relay(p + 1)
        if p == side:
            down.forward()
        if side <= p < count + side:
            gather.forward(p - side)
        if p >= 2 * side:
            gather.corner(p - 2 * side)
        if p == side + 2:
            second.begin()
        if p == 3 * side:
            down.corner()
            second.relay(0)
    second.local_copy()
    gather.finish()
    down.finish()
    for p in range(side):
        second.arrived(p)
    gather.drain()
    down.drain()
    first.finish()
    second.finish()


def gather_weights(src_one, down_src, gate_two, up_two, gain):
    side = lax.axis_size("tp")
    two, rows, width = src_one.shape
    full = jax.ShapeDtypeStruct((two, rows * side, width), src_one.dtype)
    down = jax.ShapeDtypeStruct((side, *down_src.shape), down_src.dtype)
    return pl.pallas_call(
        weights_kernel,
        out_shape=(full, down, full),
        in_specs=[ANY, ANY, ANY, ANY, VMEM],
        out_specs=(ANY,) * 3,
        scratch_shapes=[
            pltpu.VMEM((two, rows, width), gate_two.dtype),
            pltpu.VMEM((two, rows, width), src_one.dtype),
            pltpu.VMEM((rows // 4, width), src_one.dtype),
            pltpu.VMEM(down_src.shape, down_src.dtype),
            pltpu.VMEM((two, rows // 4, width), src_one.dtype),
            pltpu.VMEM((two, rows // 4, width), src_one.dtype),
            pltpu.SemaphoreType.DMA((3, first_cuts, side)),
            pltpu.SemaphoreType.DMA((3, first_cuts)),
            pltpu.SemaphoreType.DMA((3, 1, side)),
            pltpu.SemaphoreType.DMA((3, 1)),
            pltpu.SemaphoreType.DMA((2, first_cuts, side, PlaneGather.kinds)),
            pltpu.SemaphoreType.DMA((2, DownGather.kinds)),
            pltpu.SemaphoreType.DMA((5,)),
        ],
        compiler_params=pltpu.CompilerParams(
            has_side_effects=True, vmem_limit_bytes=48 * 1024 * 1024
        ),
        name="gather_weights",
    )(src_one, down_src, gate_two, up_two, gain)


def gate_part(rows, w_in, j, hidden):
    act = jnp.dot(rows, w_in[j], preferred_element_type=jnp.float32)
    gate_act, up_act = act[:, :lane], act[:, lane:]
    value = gate_act / (1.0 + jnp.exp(-gate_act)) * up_act
    hidden[:, pl.ds(pl.multiple_of(j * lane, lane), lane)] = value.astype(jnp.bfloat16)


def compute_kernel(
    tokens, w, down, terms, gate_out, up_out, down_out,
    rows_in, w_in, down_in, hidden, terms_in, sems,
):
    groups = w.shape[2] // lane
    wide = 4 * lane
    spans = down_out.shape[1] // wide
    parts, unused, cols = down.shape

    def w_load(which, j):
        return pltpu.make_async_copy(
            w.at[which, :, pl.ds(pl.multiple_of(j * lane, lane), lane)],
            w_in.at[j, :, pl.ds(which * lane, lane)],
            sems.at[which, j],
        )

    def w_store(which, j):
        return pltpu.make_async_copy(
            w_in.at[j, :, pl.ds(which * lane, lane)],
            (gate_out, up_out)[which].at[:, pl.ds(pl.multiple_of(j * lane, lane), lane)],
            sems.at[2 + which, j],
        )

    take_rows = pltpu.make_async_copy(tokens, rows_in, sems.at[4, 0])
    take_down = [
        pltpu.make_async_copy(
            down.at[i], down_in.at[:, pl.ds(i * cols, cols)], sems.at[4, 3 + i]
        )
        for i in range(parts)
    ]
    give_down = pltpu.make_async_copy(down_in, down_out, sems.at[4, 1])
    take_rows.start()

    @pl.loop(0, groups)
    def _(j):
        w_load(0, j).start()
        w_load(1, j).start()

    for copy in take_down:
        copy.start()
    take_rows.wait()

    @pl.loop(0, groups)
    def _(j):
        w_load(0, j).wait()
        w_load(1, j).wait()
        w_store(0, j).start()
        w_store(1, j).start()

        gate_part(rows_in[...], w_in, j, hidden)

    for copy in take_down:
        copy.wait()
    give_down.start()

    @pl.loop(0, spans)
    def _(n):
        cols = pl.ds(pl.multiple_of(n * wide, wide), wide)

        terms_in[:, cols] = jnp.dot(
            hidden[...], down_in[:, cols], preferred_element_type=jnp.float32
        ).astype(jnp.bfloat16)

    give_terms = pltpu.make_async_copy(terms_in, terms, sems.at[4, 2])
    give_terms.start()

    @pl.loop(0, groups)
    def _(j):
        w_store(0, j).wait()
        w_store(1, j).wait()

    give_down.wait()
    give_terms.wait()


def compute_terms(tokens, w, down):
    two, depth, width = w.shape
    count = tokens.shape[0]
    groups = width // lane
    parts, down_rows, cols = down.shape
    down_shape = (down_rows, parts * cols)
    proj = jax.ShapeDtypeStruct((depth, width), w.dtype)
    flops = 2 * count * depth * width * 3
    return pl.pallas_call(
        compute_kernel,
        out_shape=(
            jax.ShapeDtypeStruct((count, parts * cols), jnp.bfloat16),
            proj,
            proj,
            jax.ShapeDtypeStruct(down_shape, down.dtype),
        ),
        in_specs=[ANY] * 3,
        out_specs=(ANY,) * 4,
        scratch_shapes=[
            pltpu.VMEM(tokens.shape, tokens.dtype),
            pltpu.VMEM((groups, depth, 2 * lane), w.dtype),
            pltpu.VMEM(down_shape, down.dtype),
            pltpu.VMEM((count, width), jnp.bfloat16),
            pltpu.VMEM((count, parts * cols), jnp.bfloat16),
            pltpu.SemaphoreType.DMA((5, max(groups, 3 + parts))),
        ],
        compiler_params=pltpu.CompilerParams(vmem_limit_bytes=56 * 1024 * 1024),
        cost_estimate=pl.CostEstimate(flops=flops, bytes_accessed=6 * w.size, transcendentals=0),
        name="compute_terms",
    )(tokens, w, down)


class LineSum:
    kinds = 6

    def __init__(self, here, terms, place, from_outer, from_inner, from_middle, to_inner, to_outer, sems):
        self.h, self.terms, self.place = here, terms, place
        self.from_outer, self.from_inner, self.from_middle = from_outer, from_inner, from_middle
        self.to_inner, self.to_outer, self.sems = to_inner, to_outer, sems
        self.own = terms.shape[0] // (here.last + 1)
        self.size = self.own // steps

    def term(self, mirrored, s):
        return self.place(self.h.owner(mirrored), s)

    def at(self, s):
        return pl.ds(pl.multiple_of(s * self.size, self.size), self.size)

    def copy(self, src, dst, kind, s, device):
        return remote(src, dst, self.sems.at[0, kind, s], self.sems.at[1, kind, s], device)

    def start_copy(self, o, s):
        slot = 3 - o
        return self.copy(
            self.terms.at[self.term(o, s)], self.from_outer.at[slot, self.at(s)], slot, s,
            self.h.inner,
        )

    def middle_copy(self, o, s):
        slot = 3 - o
        return self.copy(
            self.to_inner.at[slot, self.at(s)], self.from_middle.at[slot, self.at(s)], 3 + slot,
            s, self.h.inner,
        )

    def back_copy(self, s):
        return self.copy(
            self.to_outer.at[self.at(s)], self.from_inner.at[self.at(s)], 5, s, self.h.outer
        )

    def send_start(self, s):
        for o in (3, 2, 1):
            self.start_copy(o, s).start()

    def relay(self, s):
        at = self.at(s)
        for o in (3, 2):
            slot = 3 - o
            self.start_copy(o, s).wait_recv()
            self.to_inner[slot, at, :] = (
                self.from_outer[slot, at, :].astype(jnp.float32)
                + self.terms[self.term(o, s), :].astype(jnp.float32)
            ).astype(jnp.bfloat16)
            self.middle_copy(o, s).start()

    def relay_back(self, s):
        at = self.at(s)
        self.middle_copy(3, s).wait_recv()
        self.to_outer[at, :] = (
            self.from_middle[0, at, :].astype(jnp.float32)
            + self.terms[self.term(0, s), :].astype(jnp.float32)
        ).astype(jnp.bfloat16)
        self.back_copy(s).start()

    def inner_total(self, s):
        at = self.at(s)
        self.start_copy(1, s).wait_recv()
        self.middle_copy(2, s).wait_recv()
        return (
            self.from_outer[2, at, :].astype(jnp.float32)
            + self.terms[self.term(1, s), :].astype(jnp.float32)
        ) + self.from_middle[1, at, :].astype(jnp.float32)

    def end_total(self, s):
        at = self.at(s)
        self.back_copy(s).wait_recv()
        return self.terms[self.term(0, s), :].astype(jnp.float32) + self.from_inner[
            at, :
        ].astype(jnp.float32)

    def finish_end(self, s):
        for o in (3, 2, 1):
            self.start_copy(o, s).wait_send()

    def finish_inner(self, s):
        self.middle_copy(3, s).wait_send()
        self.middle_copy(2, s).wait_send()
        self.back_copy(s).wait_send()


def line_scratch(own, width):
    def rows(*lead):
        return pltpu.VMEM((*lead, own, width), jnp.bfloat16)

    return [
        rows(3), rows(), rows(2), rows(2), rows(),
        pltpu.SemaphoreType.DMA((2, LineSum.kinds, steps)),
    ]


class LineSpread:
    kinds = 6

    def __init__(self, here, out, place, sems):
        self.h, self.out, self.place, self.sems = here, out, place, sems

    def copy(self, mirrored, kind, s, device):
        rows = self.out.at[self.place(self.h.owner(mirrored), s)]
        return remote(
            rows, rows, self.sems.at[0, kind, s], self.sems.at[1, kind, s], device
        )

    def in_zero(self, s):
        return self.copy(0, 0, s, self.h.inner)

    def cross_one(self, s):
        return self.copy(1, 1, s, self.h.inner)

    def cross_zero(self, s):
        return self.copy(0, 2, s, self.h.inner)

    def out_any(self, o, s):
        return self.copy(o, 2 + o, s, self.h.outer)

    def hand_on(self, s):
        self.in_zero(s).wait_recv()
        self.cross_zero(s).start()
        self.copy(2, 1, s, self.h.inner).wait_recv()
        self.out_any(2, s).start()
        self.copy(3, 2, s, self.h.inner).wait_recv()
        self.out_any(3, s).start()

    def finish_inner(self, s):
        self.cross_one(s).wait_send()
        self.cross_zero(s).wait_send()
        for o in (1, 2, 3):
            self.out_any(o, s).wait_send()


halves = 2


def blocks_kernel(
    terms_one, tokens, gain, w_in, down_src, result, w, down,
    own_rows, normed, terms_two, hidden, w_held, down_held, down_bounce,
    outer_one, inner_one, middle_one, to_inner_one, to_outer_one, line_one,
    outer_two, inner_two, middle_two, to_inner_two, to_outer_two, line_two,
    spread_sems, plane_sems, down_sems, local, load_sems,
):
    h = Here()
    own, size = result.shape[0], result.shape[0] // steps
    count = normed.shape[0]
    half, per = count // halves, steps // halves
    is_end, is_inner = h.end == 0, h.end == 1

    def span(first, length):
        return pl.ds(pl.multiple_of(first, size), length)

    def plain_place(owner, s):
        return span(owner * own + s * size, size)

    def half_place(owner, s):
        return span((s // per) * half + owner * (own // halves) + (s % per) * size, size)

    one = LineSum(
        h, terms_one, plain_place, outer_one, inner_one, middle_one, to_inner_one, to_outer_one,
        line_one,
    )
    two = LineSum(
        h, terms_two, half_place, outer_two, inner_two, middle_two, to_inner_two, to_outer_two,
        line_two,
    )
    spread = LineSpread(h, normed, half_place, spread_sems)
    gather = PlaneGather(h, w, plane_sems, second_cuts, 1)
    down_part = DownGather(h, down_src, down, down_sems, down_bounce, local)
    take = pltpu.make_async_copy(tokens.at[span(h.f * own, own)], own_rows, local.at[2])
    take.start()

    @pl.when(is_end)
    def _():
        one.send_start(0)

    for p in range(gather.count):
        gather.own(p)
    down_part.begin()
    down_part.place()
    take.wait()

    def keep_one(s, total):
        at = pl.ds(s * size, size)
        normed[half_place(h.f, s), :] = plain_norm(
            deep_alpha * own_rows[at, :].astype(jnp.float32) + half_step * total
        ).astype(jnp.bfloat16)

    def keep_two(s, total):
        residual = deep_alpha * gain[...] * normed[half_place(h.f, s), :].astype(jnp.float32)
        result[pl.ds(s * size, size), :] = plain_norm(residual + half_step * total).astype(
            jnp.bfloat16
        )

    groups = w.shape[2] // lane
    wide = 4 * lane

    def w_load(which, j):
        return pltpu.make_async_copy(
            w.at[which, :, pl.ds(pl.multiple_of(j * lane, lane), lane)],
            w_held.at[j, :, pl.ds(which * lane, lane)],
            load_sems.at[which, j],
        )

    cols = down.shape[2]
    down_load = [
        pltpu.make_async_copy(
            down.at[i], down_held.at[:, pl.ds(i * cols, cols)], local.at[3 + i]
        )
        for i in range(h.side)
    ]

    def load():
        gather.finish()
        down_part.finish()

        @pl.loop(0, groups)
        def _(j):
            w_load(0, j).start()
            w_load(1, j).start()

        for copy in down_load:
            copy.start()

    def hide(part, first, last, wait=False):
        rows = normed.at[pl.ds(part * half, half)]

        @pl.loop(first, last)
        def _(j):
            if wait:
                w_load(0, j).wait()
                w_load(1, j).wait()
            gate_part(rows[...], w_held, j, hidden)

    def sink(part):
        @pl.loop(0, down_held.shape[1] // wide)
        def _(n):
            cols = pl.ds(pl.multiple_of(n * wide, wide), wide)
            terms_two[pl.ds(part * half, half), cols] = jnp.dot(
                hidden[...], down_held[:, cols], preferred_element_type=jnp.float32
            ).astype(jnp.bfloat16)

    def spread_end(first, last):
        @pl.when(is_end)
        def _():
            for s in range(first, last):
                for o in (1, 2, 3):
                    spread.out_any(o, s).wait_recv()

    def send_two(first, last):
        @pl.when(is_end)
        def _():
            for s in range(first, last):
                two.send_start(s)

    def relay_two(s):
        @pl.when(is_inner)
        def _():
            two.relay(s)
            two.relay_back(s)
            keep_two(s, two.inner_total(s))

    def forward(first, last):
        return [lambda p=p: gather.forward(p) for p in range(first, last)]

    def corner(first, last):
        return [lambda p=p: gather.corner(p) for p in range(first, last)]

    cut = (groups + 1) // 2
    third = (groups + 3) // 4
    jobs = {
        1: forward(0, 1),
        2: forward(1, 2),
        3: forward(2, 4),
        4: forward(4, 5),
        5: forward(5, 6),
        6: forward(6, 8),
        7: [down_part.forward, *corner(0, 2)],
        8: corner(2, 4),
        9: corner(4, 6),
        10: corner(6, 8),
        12: [down_part.corner, load],
        13: [lambda: spread_end(0, per), lambda: hide(0, 0, third, True)],
        14: [lambda: hide(0, third, 2 * third, True)],
        15: [lambda: hide(0, 2 * third, groups, True)],
    }

    def other(slot):
        for job in jobs.get(slot, ()):
            job()

    for s in range(steps):

        @pl.when(is_inner)
        def _():
            one.relay(s)

        @pl.when(is_end)
        def _():
            if s + 1 < steps:
                one.send_start(s + 1)

        other(4 * s)

        @pl.when(is_inner)
        def _():
            one.relay_back(s)

        other(4 * s + 1)

        @pl.when(is_inner)
        def _():
            keep_one(s, one.inner_total(s))
            spread.cross_one(s).start()
            spread.out_any(1, s).start()

        @pl.when(is_end)
        def _():
            keep_one(s, one.end_total(s))
            spread.in_zero(s).start()

        other(4 * s + 2)
        if s >= 1:

            @pl.when(is_inner)
            def _():
                spread.hand_on(s - 1)

        other(4 * s + 3)

    @pl.when(is_inner)
    def _():
        spread.hand_on(steps - 1)

    for copy in down_load:
        copy.wait()
    sink(0)
    send_two(0, per)
    spread_end(per, steps)
    hide(1, 0, cut)
    relay_two(0)
    hide(1, cut, groups)
    relay_two(1)
    sink(1)
    send_two(per, steps)
    for s in range(2, steps):
        relay_two(s)

    @pl.when(is_end)
    def _():
        for s in range(steps):
            keep_two(s, two.end_total(s))

    gather.drain()
    down_part.drain()
    for s in range(steps):

        @pl.when(is_end)
        def _():
            one.finish_end(s)
            two.finish_end(s)
            spread.in_zero(s).wait_send()

        @pl.when(is_inner)
        def _():
            one.finish_inner(s)
            two.finish_inner(s)
            spread.finish_inner(s)


def blocks(terms, tokens, gain, w, down_src):
    side = lax.axis_size("tp")
    count, width = terms.shape
    own = count // lax.axis_size("fs")
    two, depth, hidden = w.shape
    groups = hidden // lane
    down_rows, cols = down_src.shape
    return pl.pallas_call(
        blocks_kernel,
        out_shape=(
            jax.ShapeDtypeStruct((own, width), jnp.bfloat16),
            jax.ShapeDtypeStruct(w.shape, w.dtype),
            jax.ShapeDtypeStruct((side, down_rows, cols), down_src.dtype),
        ),
        in_specs=[VMEM, ANY, VMEM, ANY, ANY],
        out_specs=(VMEM, ANY, ANY),
        input_output_aliases={3: 1},
        scratch_shapes=[
            pltpu.VMEM((own, width), jnp.bfloat16),
            pltpu.VMEM((count, width), jnp.bfloat16),
            pltpu.VMEM((count, width), jnp.bfloat16),
            pltpu.VMEM((count // halves, hidden), jnp.bfloat16),
            pltpu.VMEM((groups, depth, two * lane), w.dtype),
            pltpu.VMEM((down_rows, side * cols), down_src.dtype),
            pltpu.VMEM(down_src.shape, down_src.dtype),
            *line_scratch(own, width),
            *line_scratch(own, width),
            pltpu.SemaphoreType.DMA((2, LineSpread.kinds, steps)),
            pltpu.SemaphoreType.DMA((2, second_cuts, side, PlaneGather.kinds)),
            pltpu.SemaphoreType.DMA((2, DownGather.kinds)),
            pltpu.SemaphoreType.DMA((3 + side,)),
            pltpu.SemaphoreType.DMA((2, groups)),
        ],
        compiler_params=pltpu.CompilerParams(
            has_side_effects=True, vmem_limit_bytes=63 * 1024 * 1024
        ),
        name="sum_norm_blocks",
    )(terms, tokens, gain, w, down_src)


emit_cuts = 8


def emit_kernel(w, down, gate_out, up_out, down_out, w_held, down_held, sems):
    rows = w.shape[1] // emit_cuts
    parts, unused, cols = down.shape
    moves = []
    for i in range(parts):
        at = pl.ds(i * cols, cols)
        moves.append((down.at[i], down_held.at[:, at], down_out.at[:, at]))
    for i in range(emit_cuts):
        at = pl.ds(i * rows, rows)
        for which, out in enumerate((gate_out, up_out)):
            moves.append((w.at[which, at], w_held.at[which, at], out.at[at]))
    takes = [pltpu.make_async_copy(m[0], m[1], sems.at[0, i]) for i, m in enumerate(moves)]
    gives = [pltpu.make_async_copy(m[1], m[2], sems.at[1, i]) for i, m in enumerate(moves)]
    for take in takes:
        take.start()
    for take, give in zip(takes, gives):
        take.wait()
        give.start()
    for give in gives:
        give.wait()


def emit(w, down):
    two, depth, width = w.shape
    parts, down_rows, cols = down.shape
    proj = jax.ShapeDtypeStruct((depth, width), w.dtype)
    down_shape = (down_rows, parts * cols)
    return pl.pallas_call(
        emit_kernel,
        out_shape=(proj, proj, jax.ShapeDtypeStruct(down_shape, down.dtype)),
        in_specs=[ANY] * 2,
        out_specs=(ANY,) * 3,
        scratch_shapes=[
            pltpu.VMEM(w.shape, w.dtype),
            pltpu.VMEM(down_shape, down.dtype),
            pltpu.SemaphoreType.DMA((2, two * emit_cuts + parts)),
        ],
        compiler_params=pltpu.CompilerParams(vmem_limit_bytes=56 * 1024 * 1024),
        name="emit_projections",
    )(w, down)


def body(prompt, gate_first, up_first, down_first, norm_gain, gate_second, up_second, down_second):
    side, groups, planes = lax.axis_size("tp"), lax.axis_size("grp"), lax.axis_size("fs")
    fs_index = lax.axis_index("fs")
    tokens = prompt.reshape(-1, prompt.shape[-1])
    row_block, width = gate_first.shape
    gain_rows = lax.dynamic_slice_in_dim(norm_gain, fs_index * row_block, row_block, 0)[:, None]
    down_a, down_b = down_first.astype(jnp.bfloat16), down_second.astype(jnp.bfloat16)
    planar = (
        groups == 2
        and side == 2 * groups
        and planes == side
        and row_block % (4 * 64) == 0
        and width % lane == 0
        and down_first.shape[0] % 32 == 0
        and down_first.shape[1] % lane == 0
        and tokens.shape[0] % (planes * steps * 16) == 0
        and tokens.shape[0] % (halves * planes * 16) == 0
        and tokens.shape[1] % (4 * lane) == 0
    )
    if planar:
        src_one = jnp.stack([gate_first.astype(jnp.bfloat16), up_first.astype(jnp.bfloat16)])
        w_one, down_one, w_two = gather_weights(
            src_one, down_a, gate_second, up_second, gain_rows
        )
        terms_one, gate_one, up_one, down_one = compute_terms(tokens, w_one, down_one)
        result, w_two, down_two = blocks(terms_one, tokens, norm_gain[None, :], w_two, down_b)
        gate_two, up_two, down_two = emit(w_two, down_two)
    else:
        result, gate_one, up_one, down_one, gate_two, up_two, down_two = general_blocks(
            tokens,
            norm_gain,
            (gate_first.astype(jnp.bfloat16), up_first.astype(jnp.bfloat16), down_a),
            (
                (gain_rows * gate_second).astype(jnp.bfloat16),
                (gain_rows * up_second).astype(jnp.bfloat16),
                down_b,
            ),
        )
    return (
        result.reshape(1, result.shape[0], result.shape[-1]),
        gate_one,
        up_one,
        down_one,
        gate_two,
        up_two,
        down_two,
    )


def solution(mesh):
    placed = (
        P(("grp", "tp"), None, None),
        P("fs", "tp"),
        P("fs", "tp"),
        P("fs", "tp"),
        P(),
        P("fs", "tp"),
        P("fs", "tp"),
        P("fs", "tp"),
    )
    return jax.shard_map(
        body,
        mesh=mesh,
        in_specs=placed,
        out_specs=(
            P(("grp", "tp"), "fs", None),
            P("grp", "fs"),
            P("grp", "fs"),
            P("fs", "grp"),
            P("grp", "fs"),
            P("grp", "fs"),
            P("fs", "grp"),
        ),
        check_vma=False,
    )
```
